32 devices in a mesh: fs: 4 (over y, x), tp: 8 (over z, core).
Axes of the slice: x: 2, y: 2, z: 4, core: 2. Of those that a mesh axis runs over, the one named last changes fastest.
Arguments:
- tokens: bfloat16 [512, 4096], P('fs', 'tp'), may hold values from -6 to 6
- expert_ids: int32 [512, 8], P('fs'), may hold values from 0 to 63, all different within a row; in each aligned block of 128 rows (0 to 127, 128 to 255, ...) at most 32 rows name the same one
- affinity: float32 [512, 8], P('fs'), may hold values from 0.05 to 1
- norm_gain: float32 [4096], P('fs'), may hold values from 0.1 to 1.9
- gate_train: float32 [64, 512, 4096], P(None, 'tp', 'fs'), may hold values from -0.09375 to 0.09375
- up_train: float32 [64, 512, 4096], P(None, 'tp', 'fs'), may hold values from -0.09375 to 0.09375
- down_train: float32 [64, 512, 4096], P(None, 'fs', 'tp'), may hold values from -0.25 to 0.25
- shared_gate_train: float32 [512, 4096], P('tp', 'fs'), may hold values from -0.09375 to 0.09375
- shared_up_train: float32 [512, 4096], P('tp', 'fs'), may hold values from -0.09375 to 0.09375
- shared_down_train: float32 [512, 4096], P('fs', 'tp'), may hold values from -0.25 to 0.25
Outputs:
- mixed: bfloat16 [512, 4096], P('fs', 'tp')
- gate_serve: bfloat16 [64, 512, 4096], P('fs', 'tp')
- up_serve: bfloat16 [64, 512, 4096], P('fs', 'tp')
- down_serve: bfloat16 [64, 512, 4096], P('fs', None, 'tp')
- shared_gate_serve: bfloat16 [512, 4096], P('tp')
- shared_up_serve: bfloat16 [512, 4096], P('tp')
- shared_down_serve: bfloat16 [512, 4096], P(None, 'tp')
The draws below stay inside these ranges and needn't reach their ends.
Inputs may be any that keep to these rules, and one draw needn't show every extreme that they name: `expert_ids`: each row names 8 different experts. In each aligned block of 128 rows (the tokens of one index of fs) no expert is named by more than 32 rows, a bound that some block reaches.
All inputs are finite; a program needn't handle non-finite values.
Results may differ from the reference program's by a relative error of at most 0.019.
Values may be sent and summed in bfloat16 or wider, within the bound.
No kernel may reach another device: no remote copies, remote signals or barrier semaphores. Data moves between devices by JAX's collectives and lax.ppermute only.
A program may use at most 192 MiB of HBM per device.

```python
import math
import jax
import jax.numpy as jnp
import numpy as np
from jax import lax

D = 4096
H = 512
EXPERTS = 64
K = 8
TOK = 128
CAP = 32
TOKENS = 512
N_FS = 4


def block_scale(own_key, dims, cuts, smallest, high):
    level = 1.0
    for dim, shards_of in cuts:
        heights = jax.random.uniform(jax.random.fold_in(jax.random.fold_in(own_key, 6), dim), (shards_of,), jnp.float32, smallest / len(cuts), high / len(cuts))
        level = level * jnp.repeat(jnp.exp(heights), dims[dim] // shards_of).reshape((-1,) + (1,) * (len(dims) - 1 - dim))
    return level


def assign_block(stream_key, own, number, rows, amount, top, reach, lean):
    order = jax.random.permutation(stream_key, amount)
    packed, usual = shares(amount, rows * top, reach, lean, True), shares(amount, rows * top, reach, lean, False)
    places = jnp.arange(amount)

    def named(tallies, rotation):
        used = int((tallies > 0).sum())
        fixed = max(1, used // 4)
        moved = fixed + (places - fixed + rotation * (used - fixed)) % max(1, amount - fixed)
        return jnp.zeros((amount,), jnp.int32).at[order[jnp.where(places < fixed, places, moved)]].set(jnp.asarray(tallies, jnp.int32))

    tallies = jnp.where(number % 4 == 0, named(packed, number // 4), named(usual, number - number // 4 - 1))
    mixed = jax.random.permutation(jax.random.fold_in(own, 3), amount)
    giver, taker = mixed[0:amount // 2 * 2:2], mixed[1:amount // 2 * 2:2]
    slack = jnp.minimum(tallies[giver] - 1, reach - tallies[taker]) // 2
    slack = jnp.where((giver == order[0]) | (taker == order[0]) | (tallies[taker] == 0), 0, jnp.maximum(slack, 0))
    moved = jax.random.randint(jax.random.fold_in(own, 4), (amount // 2,), 0, 1 << 20) % (slack + 1)
    tallies = tallies.at[giver].add(-moved).at[taker].add(moved)
    items = jnp.searchsorted(jnp.cumsum(tallies), jnp.arange(rows * top), side="right").astype(jnp.int32)
    table = items.reshape(top, rows).T
    table = table[jax.random.permutation(jax.random.fold_in(own, 1), rows)]
    rotation = jax.random.randint(jax.random.fold_in(own, 2), (rows, 1), 0, top)
    return jnp.take_along_axis(table, (jnp.arange(top)[None, :] + rotation) % top, axis=1)


def shares(count, total, limit, lean, full):
    portions = [(1 << 20) // math.isqrt(rank ** lean) + 1 for rank in range(1, count + 1)]
    largest = limit if full else min(limit, max(-(-total // count), total * portions[0] // sum(portions)))
    least = 1 if total - largest >= count - 1 else 0
    holding, spare = [largest] + [least] * (count - 1), total - largest - least * (count - 1)
    while spare > 0:
        free = [i for i in range(1, count) if holding[i] < largest] or [i for i in range(1, count) if holding[i] < limit]
        whole, left = sum([portions[i] for i in free]), spare
        for i in free:
            more = min(limit - holding[i], max(1, left * portions[i] // whole), spare)
            holding[i] = holding[i] + more
            spare = spare - more
    return np.array(holding)


def bell_draw(key, extent, scale, limit, pieces=(), kind=jnp.bfloat16):
    result = scale * jax.random.normal(key, extent, jnp.float32)
    if pieces:
        result = result * block_scale(key, extent, pieces, -0.22, 0.18)
    return jnp.clip(result, -limit, limit).astype(kind)


def setup_inputs(seed: int = 0) -> dict:
    seeds = jax.random.split(jax.random.key(seed), 11)
    tokens = bell_draw(seeds[0], (TOKENS, D), 1.0, 6.0, ((0, 4), (1, 8)))
    expert_ids_keys = jax.random.split(jax.random.fold_in(seeds[1], 1), TOKENS // TOK)
    expert_ids_turns = jax.random.permutation(jax.random.fold_in(seeds[1], 3), TOKENS // TOK)
    expert_ids = jax.vmap(lambda own, number: assign_block(jax.random.fold_in(seeds[1], 2), own, number, TOK, EXPERTS, K, CAP, 1))(expert_ids_keys, expert_ids_turns).reshape((TOKENS, K))
    affinity = jnp.clip(0.05 + 0.95 * jax.random.uniform(seeds[2], (TOKENS, K), jnp.float32) ** block_scale(seeds[2], (TOKENS, K), ((0, 4),), -0.2, 0.2), 0.05, 1.0)
    norm_gain = jnp.clip(1.0 + 0.18 * jax.random.normal(seeds[3], (D,), jnp.float32), 0.1, 1.9)
    gate_train = bell_draw(seeds[4], (EXPERTS, H, D), D ** -0.5, 0.09375, ((1, 8), (2, 4)), jnp.float32)
    up_train = bell_draw(seeds[5], (EXPERTS, H, D), D ** -0.5, 0.09375, ((1, 8), (2, 4)), jnp.float32)
    down_train = bell_draw(seeds[6], (EXPERTS, H, D), H ** -0.5, 0.25, ((1, 4), (2, 8)), jnp.float32)
    shared_gate_train = bell_draw(seeds[7], (H, D), D ** -0.5, 0.09375, ((0, 8), (1, 4)), jnp.float32)
    shared_up_train = bell_draw(seeds[8], (H, D), D ** -0.5, 0.09375, ((0, 8), (1, 4)), jnp.float32)
    shared_down_train = bell_draw(seeds[9], (H, D), H ** -0.5, 0.25, ((0, 4), (1, 8)), jnp.float32)
    return {"tokens": tokens, "expert_ids": expert_ids, "affinity": affinity, "norm_gain": norm_gain, "gate_train": gate_train, "up_train": up_train, "down_train": down_train, "shared_gate_train": shared_gate_train, "shared_up_train": shared_up_train, "shared_down_train": shared_down_train}


norm_eps = 1e-06
routed_scale = 2.5

def reference(tokens, expert_ids, affinity, norm_gain, gate_train, up_train, down_train, shared_gate_train, shared_up_train, shared_down_train):
    gain_cols = norm_gain[None, None, :]
    gate_serve = (gate_train * gain_cols).astype(jnp.bfloat16)
    up_serve = (up_train * gain_cols).astype(jnp.bfloat16)
    down_serve = down_train.astype(jnp.bfloat16)
    shared_gate_serve = (shared_gate_train * norm_gain[None, :]).astype(jnp.bfloat16)
    shared_up_serve = (shared_up_train * norm_gain[None, :]).astype(jnp.bfloat16)
    shared_down_serve = shared_down_train.astype(jnp.bfloat16)
    widened = tokens.astype(jnp.float32)
    inverse_rms = lax.rsqrt(lax.optimization_barrier(jnp.mean(widened * widened, axis=1)) + norm_eps)
    shared_gate = jnp.dot(tokens, shared_gate_serve.T, preferred_element_type=jnp.float32) * inverse_rms[:, None]
    shared_up = jnp.dot(tokens, shared_up_serve.T, preferred_element_type=jnp.float32) * inverse_rms[:, None]
    shared_hidden = (jax.nn.silu(shared_gate) * shared_up).astype(jnp.bfloat16)
    shared_out = jnp.dot(shared_hidden, shared_down_serve, preferred_element_type=jnp.float32)
    ids = expert_ids.reshape(N_FS, TOK * K)
    onehot = (ids[:, :, None] == jnp.arange(EXPERTS, dtype=jnp.int32)[None, None, :]).astype(jnp.int32)
    slot_index = lax.optimization_barrier(jnp.sum((jnp.cumsum(onehot, axis=1) - onehot) * onehot, axis=2))
    block_index = jnp.arange(N_FS, dtype=jnp.int32)[:, None]
    position = (ids * (N_FS * CAP) + block_index * CAP + slot_index).reshape(-1).astype(jnp.int32)
    token_of = jnp.repeat(jnp.arange(TOKENS, dtype=jnp.int32), K)
    rows = jnp.zeros((EXPERTS * N_FS * CAP, D), jnp.bfloat16).at[position].set(tokens[token_of])
    scales = jnp.zeros((EXPERTS * N_FS * CAP,), jnp.float32).at[position].set(inverse_rms[token_of])

    def one_expert(operands):
        rows_e, scale_e, gate_w, up_w, down_w = operands
        gate_pre = jnp.dot(rows_e, gate_w.T, preferred_element_type=jnp.float32) * scale_e[:, None]
        up_pre = jnp.dot(rows_e, up_w.T, preferred_element_type=jnp.float32) * scale_e[:, None]
        hidden = (jax.nn.silu(gate_pre) * up_pre).astype(jnp.bfloat16)
        return jnp.dot(hidden, down_w, preferred_element_type=jnp.float32).astype(jnp.bfloat16)
    outputs = lax.map(one_expert, (rows.reshape(EXPERTS, N_FS * CAP, D), scales.reshape(EXPERTS, N_FS * CAP), gate_serve, up_serve, down_serve))
    picked = outputs.reshape(EXPERTS * N_FS * CAP, D)[position].reshape(TOKENS, K, D).astype(jnp.float32)
    route_weight = routed_scale * affinity / lax.optimization_barrier(jnp.sum(affinity, axis=1, keepdims=True))
    routed = lax.optimization_barrier(jnp.sum(picked * route_weight[:, :, None], axis=1))
    mixed = (shared_out + routed).astype(jnp.bfloat16)
    return (mixed, gate_serve, up_serve, down_serve, shared_gate_serve, shared_up_serve, shared_down_serve)
```

```python
import functools

import jax
import jax.numpy as jnp
from jax import lax
from jax.experimental import pallas as pl
from jax.experimental.pallas import tpu as pltpu
from jax.sharding import PartitionSpec as P

K = 8
EXPERTS = 64

norm_eps = 1e-06
routed_scale = 2.5

VMEM_LIMIT = 60 * 1024 * 1024
ANY = pl.BlockSpec(memory_space=pl.ANY)
VMEM = pl.BlockSpec(memory_space=pltpu.VMEM)
SMEM = pl.BlockSpec(memory_space=pltpu.SMEM)


def partner(i, s, n):
    if n & (n - 1) == 0:
        return i ^ s, i ^ s
    return (i + s) % n, (i + n - s) % n


def exchange(x, axis, n, s):
    return lax.ppermute(x, axis, [(i, partner(i, s, n)[0]) for i in range(n)])


def give_back(x, axis, n, s):
    return lax.ppermute(x, axis, [(i, partner(i, s, n)[1]) for i in range(n)])


def cuts(count):
    marks = [0] + [-(-count * num // 16) for num in (2, 6, 11, 16)]
    return [(lo, hi - lo) for lo, hi in zip(marks, marks[1:]) if hi > lo]


def prep_gu_body(n, idx_ref, gain_ref, *refs):
    gates, ups, outs = refs[:n], refs[n : 2 * n], refs[2 * n :]
    gain = gain_ref[...]
    for s in range(n):
        outs[s][0, 0] = (gates[s][0] * gain).astype(jnp.bfloat16)
        outs[s][1, 0] = (ups[s][0] * gain).astype(jnp.bfloat16)


def prep_gu(gate, up, gain, base, lo, count):
    n = base.shape[0]
    _, hp, df = gate.shape
    block = lambda s: pl.BlockSpec((1, hp, df), lambda i, idx, s=s: (idx[s] + i, 0, 0))
    return pl.pallas_call(
        functools.partial(prep_gu_body, n),
        grid_spec=pltpu.PrefetchScalarGridSpec(
            num_scalar_prefetch=1,
            grid=(count,),
            in_specs=[pl.BlockSpec((1, df), lambda i, idx: (0, 0))]
            + [block(s) for s in range(n)] * 2,
            out_specs=[pl.BlockSpec((2, 1, hp, df), lambda i, idx: (0, i, 0, 0))] * n,
        ),
        out_shape=[jax.ShapeDtypeStruct((2, count, hp, df), jnp.bfloat16)] * n,
        compiler_params=pltpu.CompilerParams(vmem_limit_bytes=VMEM_LIMIT),
        name=f"prep_gu_{lo}",
    )(base + lo, gain, *([gate] * n), *([up] * n))


def prep_down_body(n, idx_ref, *refs):
    for s in range(n):
        refs[n + s][0] = refs[s][0].astype(jnp.bfloat16)


def prep_down(down, base, lo, count):
    n = base.shape[0]
    _, hf, dp = down.shape
    block = lambda s: pl.BlockSpec((1, hf, dp), lambda i, idx, s=s: (idx[s] + i, 0, 0))
    return pl.pallas_call(
        functools.partial(prep_down_body, n),
        grid_spec=pltpu.PrefetchScalarGridSpec(
            num_scalar_prefetch=1,
            grid=(count,),
            in_specs=[block(s) for s in range(n)],
            out_specs=[pl.BlockSpec((1, hf, dp), lambda i, idx: (i, 0, 0))] * n,
        ),
        out_shape=[jax.ShapeDtypeStruct((count, hf, dp), jnp.bfloat16)] * n,
        compiler_params=pltpu.CompilerParams(vmem_limit_bytes=VMEM_LIMIT),
        name=f"prep_down_{lo}",
    )(base + lo, *([down] * n))


def gu_body(n, lo, count, shared, first, *refs):
    refs = list(refs)
    take = lambda k: [refs.pop(0) for _ in range(k)]
    (blk_ref, x_ref, inv_ref, w_ref) = take(4)
    pieces = take(n)
    shared_pieces = take(n) if shared else []
    if not first:
        take(2)
    gate_out, up_out = take(2)
    shared_out = take(2) if shared else []
    (a_ref,) = take(1)
    buf, acc_g, acc_u, in_sem, out_sem = refs
    tot = count + (1 if shared else 0)
    hp, df = buf.shape[-2:]
    dp = x_ref.shape[-1]
    ratio = df // dp
    incoming = []
    for s in range(n):
        here = [pltpu.make_async_copy(pieces[s], buf.at[s, :, pl.ds(0, count)], in_sem.at[s, 0])]
        if shared:
            here.append(
                pltpu.make_async_copy(shared_pieces[s], buf.at[s, :, count], in_sem.at[s, 1])
            )
        for copy in here:
            copy.start()
        incoming.append(here)
    outgoing = []
    nt = (((1,), (1,)), ((), ()))
    for s in range(n):
        for copy in incoming[s]:
            copy.wait()
        blk = blk_ref[s]
        cols = pl.ds(pl.multiple_of(blk * df, df), df)
        here = []
        for m, out in enumerate((gate_out, up_out)):
            here.append(
                pltpu.make_async_copy(
                    buf.at[s, m, pl.ds(0, count)],
                    out.at[pl.ds(lo, count), :, cols],
                    out_sem.at[s, m, 0],
                )
            )
        for m, out in enumerate(shared_out):
            here.append(
                pltpu.make_async_copy(buf.at[s, m, count], out.at[:, cols], out_sem.at[s, m, 1])
            )
        for copy in here:
            copy.start()
        outgoing += here
        for m, acc in enumerate((acc_g, acc_u)):
            part = None
            for j in range(ratio):
                w = buf[s, m, :, :, j * dp : (j + 1) * dp].reshape(tot * hp, dp)
                dot = lax.dot_general(
                    x_ref[blk * ratio + j], w, nt, preferred_element_type=jnp.float32
                )
                part = dot if part is None else part + dot
            if s == 0:
                acc[...] = part
            else:
                acc[...] += part
    inv = inv_ref[...]
    w = w_ref[...]
    gate = acc_g[...] * inv
    up = acc_u[...] * inv
    hidden = gate * jax.nn.sigmoid(gate) * up
    a_ref[...] = jnp.where(w > 0, hidden * w, 0.0).astype(jnp.bfloat16)
    for copy in outgoing:
        copy.wait()


def gu_step(blk, x, inv, w, pieces, shared_pieces, prev, lo, count, n_local, width):
    n = len(pieces)
    hp, df = pieces[0].shape[-2:]
    rows = x.shape[1]
    shared = bool(shared_pieces)
    tot = count + (1 if shared else 0)
    bf = jnp.bfloat16
    out_shape = [jax.ShapeDtypeStruct((n_local, hp, width), bf)] * 2
    if shared:
        out_shape += [jax.ShapeDtypeStruct((hp, width), bf)] * 2
    out_shape.append(jax.ShapeDtypeStruct((rows, tot * hp), bf))
    args = [blk, x, inv, w, *pieces, *shared_pieces, *prev]
    specs = [SMEM, VMEM, VMEM, VMEM] + [ANY] * (len(args) - 4)
    aliases = {len(args) - 2: 0, len(args) - 1: 1} if prev else {}
    return pl.pallas_call(
        functools.partial(gu_body, n, lo, count, shared, not prev),
        in_specs=specs,
        out_specs=[ANY] * (len(out_shape) - 1) + [VMEM],
        out_shape=out_shape,
        scratch_shapes=[
            pltpu.VMEM((n, 2, tot, hp, df), bf),
            pltpu.VMEM((rows, tot * hp), jnp.float32),
            pltpu.VMEM((rows, tot * hp), jnp.float32),
            pltpu.SemaphoreType.DMA((n, 2)),
            pltpu.SemaphoreType.DMA((n, 2, 2)),
        ],
        input_output_aliases=aliases,
        compiler_params=pltpu.CompilerParams(vmem_limit_bytes=VMEM_LIMIT),
        name=f"gu_{lo}",
    )(*args)


def down_body(n, lo, count, shared, first, last, own_rows, *refs):
    refs = list(refs)
    take = lambda k: [refs.pop(0) for _ in range(k)]
    blk_ref, a_ref = take(2)
    acc_in = None if first else take(1)[0]
    pieces = take(n)
    shared_pieces = take(n) if shared else []
    if not first:
        take(1)
    (down_out,) = take(1)
    shared_out = take(1)[0] if shared else None
    results = take(n) if last else take(1)
    buf, in_sem, out_sem = refs
    tot = count + (1 if shared else 0)
    hf = pieces[0].shape[1]
    copies = []
    for s in range(n):
        rows = pl.ds(pl.multiple_of(blk_ref[s] * hf, hf), hf)
        copies.append(
            pltpu.make_async_copy(pieces[s], buf.at[pl.ds(0, count), rows], in_sem.at[s, 0])
        )
        if shared:
            copies.append(
                pltpu.make_async_copy(shared_pieces[s], buf.at[count, rows], in_sem.at[s, 1])
            )
    for copy in copies:
        copy.start()
    for copy in copies:
        copy.wait()
    copies = [
        pltpu.make_async_copy(
            buf.at[pl.ds(0, count)], down_out.at[pl.ds(lo, count)], out_sem.at[0]
        )
    ]
    if shared:
        copies.append(pltpu.make_async_copy(buf.at[count], shared_out, out_sem.at[1]))
    for copy in copies:
        copy.start()
    parts = a_ref.shape[0]
    hp = buf.shape[1] // parts
    dp = buf.shape[2]
    for r in range(n):
        at = pl.ds(r * own_rows, own_rows)
        total = None if first else acc_in[at, :]
        for p in range(parts):
            w = buf[:, p * hp : (p + 1) * hp, :].reshape(tot * hp, dp)
            dot = jnp.dot(a_ref[p, at, :], w, preferred_element_type=jnp.float32)
            total = dot if total is None else total + dot
        if last:
            results[r][...] = total.astype(results[r].dtype)
        else:
            results[0][at, :] = total
    for copy in copies:
        copy.wait()


def down_step(blk, a, acc, pieces, shared_pieces, prev, lo, count, n_local, last):
    n = len(pieces)
    _, hf, dp = pieces[0].shape
    rows = a.shape[1]
    own = rows // n
    hidden = hf * n
    shared = bool(shared_pieces)
    tot = count + (1 if shared else 0)
    first = prev is None
    bf = jnp.bfloat16
    out_shape = [jax.ShapeDtypeStruct((n_local, hidden, dp), bf)]
    if shared:
        out_shape.append(jax.ShapeDtypeStruct((hidden, dp), bf))
    n_any = len(out_shape)
    if last:
        out_shape.append(jax.ShapeDtypeStruct((own, dp), jnp.float32))
        out_shape += [jax.ShapeDtypeStruct((own, dp), bf)] * (n - 1)
    else:
        out_shape.append(jax.ShapeDtypeStruct((rows, dp), jnp.float32))
    args = [blk, a] + ([] if first else [acc])
    specs = [SMEM] + [VMEM] * (len(args) - 1)
    args += [*pieces, *shared_pieces] + ([] if first else [prev])
    specs += [ANY] * (len(args) - len(specs))
    return pl.pallas_call(
        functools.partial(down_body, n, lo, count, shared, first, last, own),
        in_specs=specs,
        out_specs=[ANY] * n_any + [VMEM] * (len(out_shape) - n_any),
        out_shape=out_shape,
        scratch_shapes=[
            pltpu.VMEM((tot, hidden, dp), bf),
            pltpu.SemaphoreType.DMA((n, 2)),
            pltpu.SemaphoreType.DMA((2,)),
        ],
        input_output_aliases={} if first else {len(args) - 1: 0},
        compiler_params=pltpu.CompilerParams(vmem_limit_bytes=VMEM_LIMIT),
        name=f"down_{lo}",
    )(*args)


def body(
    n,
    tokens,
    expert_ids,
    affinity,
    norm_gain,
    gate_train,
    up_train,
    down_train,
    shared_gate_train,
    shared_up_train,
    shared_down_train,
):
    bf = jnp.bfloat16
    me = lax.axis_index("fs")
    experts, hp, _ = gate_train.shape
    n_local = experts // n
    width = norm_gain.shape[0] * n
    to = [partner(me, s, n)[0] for s in range(n)]
    blk = jnp.stack([partner(me, s, n)[1] for s in range(n)]).astype(jnp.int32)
    base = (jnp.stack(to) * n_local).astype(jnp.int32)
    gain = norm_gain[None, :]

    swap = lambda pieces: [pieces[0]] + [exchange(pieces[s], "fs", n, s) for s in range(1, n)]

    blocks = jnp.stack(swap([tokens] * n))
    x = lax.all_gather(blocks.reshape(-1, tokens.shape[1]), "tp", axis=0)

    route_weight = routed_scale * affinity / jnp.sum(affinity, axis=1, keepdims=True)

    def weights_for(first):
        names = first + jnp.arange(n_local, dtype=jnp.int32)
        hit = expert_ids[:, :, None] == names[None, None, :]
        return jnp.sum(jnp.where(hit, route_weight[:, :, None], 0.0), axis=1)

    w = jnp.concatenate(swap([weights_for(base[s]) for s in range(n)]))

    shared_gu = swap([(jnp.stack([shared_gate_train, shared_up_train]) * gain).astype(bf)] * n)
    chunks = cuts(n_local)
    gu = [swap(prep_gu(gate_train, up_train, gain, base, lo, count)) for lo, count in chunks]
    order = list(range(1, len(chunks))) + [0]
    down = {c: swap(prep_down(down_train, base, *chunks[c])) for c in order}
    shared_down = swap([shared_down_train.astype(bf)] * n)

    rows = x.shape[1]
    wide = x.astype(jnp.float32)
    inv = lax.rsqrt(jnp.sum(wide * wide, axis=(0, 2)) / width + norm_eps)[:, None]
    own = (jnp.arange(rows) < tokens.shape[0]).astype(jnp.float32)[:, None]

    prev, gathered = [], []
    for c, (lo, count) in enumerate(chunks):
        w_here = w[:, lo : lo + count]
        if c == 0:
            w_here = jnp.concatenate([w_here, own], axis=1)
        w_here = jnp.repeat(w_here, hp, axis=1)
        results = gu_step(
            blk, x, inv, w_here, gu[c], shared_gu if c == 0 else [], prev, lo, count, n_local, width
        )
        if c == 0:
            shared_gate_serve, shared_up_serve = results[2:4]
        prev = results[:2]
        gathered.append(lax.all_gather(results[-1], "tp", axis=0))
    gate_serve, up_serve = prev

    acc, down_serve = None, None
    for c in order:
        last = c == order[-1]
        lo, count = chunks[c]
        results = down_step(
            blk,
            gathered[c],
            acc,
            down[c],
            shared_down if c == 0 else [],
            down_serve,
            lo,
            count,
            n_local,
            last,
        )
        down_serve = results[0]
        if c == 0:
            shared_down_serve = results[1]
        acc = results[-1]
    sums = results[2:]
    total = sums[0]
    for s in range(1, n):
        total = total + give_back(sums[s], "fs", n, s).astype(jnp.float32)
    return (
        total.astype(bf),
        gate_serve,
        up_serve,
        down_serve,
        shared_gate_serve,
        shared_up_serve,
        shared_down_serve,
    )


def solution(mesh):
    return jax.shard_map(
        functools.partial(body, mesh.shape["fs"]),
        mesh=mesh,
        in_specs=(
            P("fs", "tp"),
            P("fs", None),
            P("fs", None),
            P("fs"),
            P(None, "tp", "fs"),
            P(None, "tp", "fs"),
            P(None, "fs", "tp"),
            P("tp", "fs"),
            P("tp", "fs"),
            P("fs", "tp"),
        ),
        out_specs=(
            P("fs", "tp"),
            P("fs", "tp", None),
            P("fs", "tp", None),
            P("fs", None, "tp"),
            P("tp", None),
            P("tp", None),
            P(None, "tp"),
        ),
        check_vma=False,
    )
```

```python
import functools

import jax
import jax.numpy as jnp
from jax import lax
from jax.experimental import pallas as pl
from jax.experimental.pallas import tpu as pltpu
from jax.sharding import PartitionSpec as P


K = 8

norm_eps = 1e-06
routed_scale = 2.5

VMEM_LIMIT = 60 * 1024 * 1024
ANY = pl.BlockSpec(memory_space=pl.ANY)
VMEM = pl.BlockSpec(memory_space=pltpu.VMEM)
SMEM = pl.BlockSpec(memory_space=pltpu.SMEM)


def partner(i, s, n):
    if n & (n - 1) == 0:
        return i ^ s, i ^ s
    return (i + s) % n, (i + n - s) % n


def exchange(x, axis, n, s):
    return lax.ppermute(x, axis, [(i, partner(i, s, n)[0]) for i in range(n)])


def give_back(x, axis, n, s):
    return lax.ppermute(x, axis, [(i, partner(i, s, n)[1]) for i in range(n)])


def gather_z(x):
    parts = lax.axis_size("tp")
    half = parts // 2
    got = [x]
    for s in range(1, half):
        pairs = [(i, 2 * partner(i // 2, s, half)[0] + i % 2) for i in range(parts)]
        got.append(lax.ppermute(x, "tp", pairs))
    return got


def swap_core(pieces):
    parts = lax.axis_size("tp")
    return [lax.ppermute(x, "tp", [(i, i ^ 1) for i in range(parts)]) for x in pieces]


def gathered_from():
    me = lax.axis_index("tp")
    half = lax.axis_size("tp") // 2
    chips = [partner(me >> 1, s, half)[1] for s in range(half)]
    return [2 * z + core for core in (me & 1, 1 - (me & 1)) for z in chips]


def cuts(count):
    marks = [0] + [-(-count * num // 16) for num in (4, 10, 16)]
    return [(lo, hi - lo) for lo, hi in zip(marks, marks[1:]) if hi > lo]


def down_cuts(chunks):
    steps = [(c, *chunks[c]) for c in range(1, len(chunks))]
    lo, count = chunks[0]
    head = count // 2
    return steps + [(0, *part) for part in ((lo, head), (lo + head, count - head)) if part[1]]


TOKEN = jax.ShapeDtypeStruct((8, 128), jnp.float32)


def prep_gu_body(n, idx_ref, gain_ref, *refs):
    gates, ups, outs = refs[:n], refs[n : 2 * n], refs[2 * n + 1 : 3 * n + 1]
    refs[-1][...] = jnp.zeros(TOKEN.shape, TOKEN.dtype)
    gain = gain_ref[...]
    for s in range(n):
        outs[s][0, 0] = (gates[s][0] * gain).astype(jnp.bfloat16)
        outs[s][1, 0] = (ups[s][0] * gain).astype(jnp.bfloat16)


def prep_gu(gate, up, gain, base, lo, count, token):
    n = base.shape[0]
    _, hp, df = gate.shape
    block = lambda s: pl.BlockSpec((1, hp, df), lambda i, idx, s=s: (idx[s] + i, 0, 0))
    return pl.pallas_call(
        functools.partial(prep_gu_body, n),
        grid_spec=pltpu.PrefetchScalarGridSpec(
            num_scalar_prefetch=1,
            grid=(count,),
            in_specs=[pl.BlockSpec((1, df), lambda i, idx: (0, 0))]
            + [block(s) for s in range(n)] * 2
            + [ANY],
            out_specs=[pl.BlockSpec((2, 1, hp, df), lambda i, idx: (0, i, 0, 0))] * n
            + [pl.BlockSpec(TOKEN.shape, lambda i, idx: (0, 0))],
        ),
        out_shape=[jax.ShapeDtypeStruct((2, count, hp, df), jnp.bfloat16)] * n + [TOKEN],
        compiler_params=pltpu.CompilerParams(vmem_limit_bytes=VMEM_LIMIT),
    )(base + lo, gain, *([gate] * n), *([up] * n), token)


def prep_down_body(n, idx_ref, *refs):
    refs[-1][...] = jnp.zeros(TOKEN.shape, TOKEN.dtype)
    for s in range(n):
        refs[n + 1 + s][0] = refs[s][0].astype(jnp.bfloat16)


def prep_down(down, base, lo, count, token):
    n = base.shape[0]
    _, hf, dp = down.shape
    block = lambda s: pl.BlockSpec((1, hf, dp), lambda i, idx, s=s: (idx[s] + i, 0, 0))
    return pl.pallas_call(
        functools.partial(prep_down_body, n),
        grid_spec=pltpu.PrefetchScalarGridSpec(
            num_scalar_prefetch=1,
            grid=(count,),
            in_specs=[block(s) for s in range(n)] + [ANY],
            out_specs=[pl.BlockSpec((1, hf, dp), lambda i, idx: (i, 0, 0))] * n
            + [pl.BlockSpec(TOKEN.shape, lambda i, idx: (0, 0))],
        ),
        out_shape=[jax.ShapeDtypeStruct((count, hf, dp), jnp.bfloat16)] * n + [TOKEN],
        compiler_params=pltpu.CompilerParams(vmem_limit_bytes=VMEM_LIMIT),
    )(base + lo, *([down] * n), token)


def pack_body(n, *refs):
    own = refs[0].shape[0]
    for s in range(n):
        refs[-1][s * own : (s + 1) * own, :] = refs[s][...]


def pack(pieces, token):
    n = len(pieces)
    own, dp = pieces[0].shape
    return pl.pallas_call(
        functools.partial(pack_body, n),
        in_specs=[VMEM] * n + [ANY],
        out_specs=VMEM,
        out_shape=jax.ShapeDtypeStruct((n * own, dp), pieces[0].dtype),
        name="pack_tokens",
    )(*pieces, token)


def route_body(n, parts, n_local, me_ref, from_ref, *refs):
    gathered, tables, (x_ref, w_ref, inv_ref) = refs[:parts], refs[parts : parts + n], refs[parts + n :]
    own = tables[0].shape[1]
    hp = w_ref.shape[1] // n_local
    width = x_ref.shape[0] * x_ref.shape[2]
    for s in range(n):
        at = pl.ds(s * own, own)
        squares = 0.0
        for k in range(parts):
            narrow = gathered[k][at, :]
            x_ref[from_ref[k], at, :] = narrow
            wide = narrow.astype(jnp.float32)
            squares = squares + jnp.sum(wide * wide, axis=1, keepdims=True)
        inv_ref[at, :] = lax.rsqrt(squares / width + norm_eps)
        table = tables[s][...].T
        ids, affinity = table[:, :K].astype(jnp.int32), table[:, K:]
        weight = routed_scale * affinity / jnp.sum(affinity, axis=1, keepdims=True)
        for e in range(n_local):
            hit = ids == me_ref[0] * n_local + e
            here = jnp.sum(jnp.where(hit, weight, 0.0), axis=1, keepdims=True)
            w_ref[at, e * hp : (e + 1) * hp] = jnp.broadcast_to(here, (own, hp))


def route(me, source, gathered, tables, n_local, hp):
    n, parts = len(tables), len(gathered)
    rows, dp = gathered[0].shape
    return pl.pallas_call(
        functools.partial(route_body, n, parts, n_local),
        in_specs=[SMEM] * 2 + [VMEM] * (parts + n),
        out_specs=[VMEM] * 3,
        out_shape=[
            jax.ShapeDtypeStruct((parts, rows, dp), gathered[0].dtype),
            jax.ShapeDtypeStruct((rows, n_local * hp), jnp.float32),
            jax.ShapeDtypeStruct((rows, 1), jnp.float32),
        ],
        compiler_params=pltpu.CompilerParams(vmem_limit_bytes=VMEM_LIMIT),
        name="route",
    )(me, source, *gathered, *tables)


def shared_down_body(n, parts, me_ref, from_ref, *refs):
    gathered, (down_ref, acc_ref) = refs[:parts], refs[parts:]
    lanes = gathered[0].shape[1]
    share = parts // n
    hp = down_ref.shape[0] // share
    acc_ref[...] = jnp.zeros(acc_ref.shape, acc_ref.dtype)
    for k in range(parts):

        @pl.when(from_ref[k] // share == me_ref[0])
        def _(k=k):
            rows = pl.ds(pl.multiple_of((from_ref[k] % share) * hp, hp), hp)
            acc_ref[...] += jnp.dot(
                gathered[k][:, lanes - hp :], down_ref[rows, :], preferred_element_type=jnp.float32
            )


def shared_down_part(n, me, source, gathered, down):
    parts = len(gathered)
    return pl.pallas_call(
        functools.partial(shared_down_body, n, parts),
        in_specs=[SMEM] * 2 + [VMEM] * (parts + 1),
        out_specs=VMEM,
        out_shape=jax.ShapeDtypeStruct((gathered[0].shape[0], down.shape[1]), jnp.float32),
        compiler_params=pltpu.CompilerParams(vmem_limit_bytes=VMEM_LIMIT),
        name="shared_down",
    )(me, source, *gathered, down)


def stack_rows_body(n, blk_ref, *refs):
    own = refs[0].shape[0]
    for s in range(n):
        refs[-1][pl.ds(pl.multiple_of(blk_ref[s] * own, own), own), :] = refs[s][...]


def stack_rows(blk, pieces, token):
    n = len(pieces)
    own, dp = pieces[0].shape
    return pl.pallas_call(
        functools.partial(stack_rows_body, n),
        in_specs=[SMEM] + [VMEM] * n + [ANY],
        out_specs=VMEM,
        out_shape=jax.ShapeDtypeStruct((n * own, dp), pieces[0].dtype),
        name="stack_rows",
    )(blk, *pieces, token)


def gu_body(n, lo, count, shared, first, *refs):
    refs = list(refs)
    take = lambda k: [refs.pop(0) for _ in range(k)]
    (blk_ref, x_ref, inv_ref, w_ref) = take(4)
    pieces = take(n)
    shared_pieces = take(n) if shared else []
    take(1 if first else 2)
    gate_out, up_out = take(2)
    shared_out = take(2) if shared else []
    (a_ref,) = take(1)
    buf, acc_g, acc_u, in_sem, out_sem = refs
    tot = count + (1 if shared else 0)
    hp, df = buf.shape[-2:]
    dp = x_ref.shape[-1]
    ratio = df // dp
    incoming = []
    for s in range(n):
        here = [pltpu.make_async_copy(pieces[s], buf.at[s, :, pl.ds(0, count)], in_sem.at[s, 0])]
        if shared:
            here.append(
                pltpu.make_async_copy(shared_pieces[s], buf.at[s, :, count], in_sem.at[s, 1])
            )
        for copy in here:
            copy.start()
        incoming.append(here)
    outgoing = []
    nt = (((1,), (1,)), ((), ()))
    for s in range(n):
        for copy in incoming[s]:
            copy.wait()
        blk = blk_ref[s]
        cols = pl.ds(pl.multiple_of(blk * df, df), df)
        here = []
        for m, out in enumerate((gate_out, up_out)):
            here.append(
                pltpu.make_async_copy(
                    buf.at[s, m, pl.ds(0, count)],
                    out.at[pl.ds(lo, count), :, cols],
                    out_sem.at[s, m, 0],
                )
            )
        for m, out in enumerate(shared_out):
            here.append(
                pltpu.make_async_copy(buf.at[s, m, count], out.at[:, cols], out_sem.at[s, m, 1])
            )
        for copy in here:
            copy.start()
        outgoing += here
        for m, acc in enumerate((acc_g, acc_u)):
            part = None
            for j in range(ratio):
                w = buf[s, m, :, :, j * dp : (j + 1) * dp].reshape(tot * hp, dp)
                dot = lax.dot_general(
                    x_ref[blk * ratio + j], w, nt, preferred_element_type=jnp.float32
                )
                part = dot if part is None else part + dot
            if s == 0:
                acc[...] = part
            else:
                acc[...] += part
    inv = inv_ref[...]
    routed = count * hp
    for lanes in [slice(0, routed)] + ([slice(routed, routed + hp)] if shared else []):
        gate = acc_g[:, lanes] * inv
        up = acc_u[:, lanes] * inv
        hidden = gate * jax.nn.sigmoid(gate) * up
        if lanes.start == 0:
            w = w_ref[:, lo * hp : lo * hp + routed]
            hidden = jnp.where(w > 0, hidden * w, 0.0)
        a_ref[:, lanes] = hidden.astype(jnp.bfloat16)
    for copy in outgoing:
        copy.wait()


def gu_step(blk, x, inv, w, pieces, shared_pieces, prev, token, lo, count, n_local, width):
    n = len(pieces)
    hp, df = pieces[0].shape[-2:]
    rows = x.shape[1]
    shared = bool(shared_pieces)
    tot = count + (1 if shared else 0)
    bf = jnp.bfloat16
    out_shape = [jax.ShapeDtypeStruct((n_local, hp, width), bf)] * 2
    if shared:
        out_shape += [jax.ShapeDtypeStruct((hp, width), bf)] * 2
    out_shape.append(jax.ShapeDtypeStruct((rows, tot * hp), bf))
    args = [blk, x, inv, w, *pieces, *shared_pieces, *(prev or [token])]
    specs = [SMEM, VMEM, VMEM, VMEM] + [ANY] * (len(args) - 4)
    aliases = {len(args) - 2: 0, len(args) - 1: 1} if prev else {}
    return pl.pallas_call(
        functools.partial(gu_body, n, lo, count, shared, not prev),
        in_specs=specs,
        out_specs=[ANY] * (len(out_shape) - 1) + [VMEM],
        out_shape=out_shape,
        scratch_shapes=[
            pltpu.VMEM((n, 2, tot, hp, df), bf),
            pltpu.VMEM((rows, tot * hp), jnp.float32),
            pltpu.VMEM((rows, tot * hp), jnp.float32),
            pltpu.SemaphoreType.DMA((n, 2)),
            pltpu.SemaphoreType.DMA((n, 2, 2)),
        ],
        input_output_aliases=aliases,
        compiler_params=pltpu.CompilerParams(vmem_limit_bytes=VMEM_LIMIT),
    )(*args)


def down_body(n, parts, lo, count, skip, first, last, *refs):
    refs = list(refs)
    take = lambda k: [refs.pop(0) for _ in range(k)]
    from_ref, blk_ref = take(2)
    gathered = take(parts)
    (acc_in,) = take(1)
    pieces = take(n)
    if not first:
        take(1)
    (down_out,) = take(1)
    results = take(n) if last else take(1)
    buf, in_sem, out_sem = refs
    hf = pieces[0].shape[1]
    copies = []
    for s in range(n):
        rows = pl.ds(pl.multiple_of(blk_ref[s] * hf, hf), hf)
        copies.append(pltpu.make_async_copy(pieces[s], buf.at[:, rows], in_sem.at[s]))
    for copy in copies:
        copy.start()
    for copy in copies:
        copy.wait()
    out = pltpu.make_async_copy(buf, down_out.at[pl.ds(lo, count)], out_sem)
    out.start()
    hp = buf.shape[1] // parts
    dp = buf.shape[2]
    lanes = slice(skip * hp, (skip + count) * hp)
    own = acc_in.shape[0] // n
    for r in range(n):
        at = pl.ds(r * own, own)
        total = acc_in[at, :]
        for k in range(parts):
            hidden = pl.ds(pl.multiple_of(from_ref[k] * hp, hp), hp)
            w = buf[:, hidden, :].reshape(count * hp, dp)
            total += jnp.dot(gathered[k][at, lanes], w, preferred_element_type=jnp.float32)
        if last:
            results[r][...] = total.astype(results[r].dtype)
        else:
            results[0][at, :] = total
    out.wait()


def down_step(source, blk, gathered, acc, pieces, prev, lo, count, skip, n_local, last):
    n, parts = len(pieces), len(gathered)
    _, hf, dp = pieces[0].shape
    rows = acc.shape[0]
    own = rows // n
    hidden = hf * n
    first = prev is None
    bf = jnp.bfloat16
    out_shape = [jax.ShapeDtypeStruct((n_local, hidden, dp), bf)]
    if last:
        out_shape.append(jax.ShapeDtypeStruct((own, dp), jnp.float32))
        out_shape += [jax.ShapeDtypeStruct((own, dp), bf)] * (n - 1)
    else:
        out_shape.append(jax.ShapeDtypeStruct((rows, dp), jnp.float32))
    args = [source, blk, *gathered, acc, *pieces] + ([] if first else [prev])
    return pl.pallas_call(
        functools.partial(down_body, n, parts, lo, count, skip, first, last),
        in_specs=[SMEM] * 2 + [VMEM] * (parts + 1) + [ANY] * (len(args) - parts - 3),
        out_specs=[ANY] + [VMEM] * (len(out_shape) - 1),
        out_shape=out_shape,
        scratch_shapes=[
            pltpu.VMEM((count, hidden, dp), bf),
            pltpu.SemaphoreType.DMA((n,)),
            pltpu.SemaphoreType.DMA,
        ],
        input_output_aliases={} if first else {len(args) - 1: 0},
        compiler_params=pltpu.CompilerParams(vmem_limit_bytes=VMEM_LIMIT),
    )(*args)


def layer(
    n,
    tokens,
    expert_ids,
    affinity,
    norm_gain,
    gate_train,
    up_train,
    down_train,
    shared_gate_train,
    shared_up_train,
    shared_down_train,
):
    bf = jnp.bfloat16
    me = lax.axis_index("fs")
    experts, hp, _ = gate_train.shape
    n_local = experts // n
    width = norm_gain.shape[0] * n
    to = [partner(me, s, n)[0] for s in range(n)]
    blk = jnp.stack([partner(me, s, n)[1] for s in range(n)]).astype(jnp.int32)
    base = (jnp.stack(to) * n_local).astype(jnp.int32)
    gain = norm_gain[None, :]

    def swap(pieces):
        return [pieces[0]] + [exchange(pieces[s], "fs", n, s) for s in range(1, n)]

    token_pieces = swap([tokens] * n)

    shared_gu = (jnp.stack([shared_gate_train, shared_up_train]) * gain).astype(bf)
    shared_gu = swap([shared_gu] * n)
    table = jnp.concatenate([expert_ids.astype(jnp.float32).T, affinity.T])
    tables = swap([table] * n)
    chunks = cuts(n_local)
    steps = down_cuts(chunks)
    token = jnp.zeros(TOKEN.shape, TOKEN.dtype)
    gu, down = {}, {}
    for c, (lo, count) in enumerate(chunks):
        *pieces, token = prep_gu(gate_train, up_train, gain, base, lo, count, token)
        gu[c] = swap(pieces)
        if c == 0:
            token = packed = pack(token_pieces, token)
            x_same = gather_z(packed)
    for i, (_, lo, count) in enumerate(steps):
        *pieces, token = prep_down(down_train, base, lo, count, token)
        down[i] = swap(pieces)
    own_shared_down = shared_down_train.astype(bf)
    shared_down = swap([own_shared_down] * n)

    x_all = x_same + swap_core(x_same)
    me = me.astype(jnp.int32)[None]
    source = jnp.stack(gathered_from()).astype(jnp.int32)
    x, w, inv = route(me, source, x_all, tables, n_local, hp)
    prev, gathered = [], []
    for c, (lo, count) in enumerate(chunks):
        results = gu_step(
            *(blk, x, inv, w, gu[c], shared_gu if c == 0 else []),
            *(prev, token, lo, count, n_local, width),
        )
        if c == 0:
            shared_gate_serve, shared_up_serve = results[2:4]
        prev = results[:2]
        same = gather_z(results[-1])
        gathered.append(same + swap_core(same))
    gate_serve, up_serve = prev

    acc = shared_down_part(n, me, source, gathered[0], own_shared_down)
    down_serve = None
    for i, (c, lo, count) in enumerate(steps):
        last = i == len(steps) - 1
        skip = lo - chunks[c][0]
        down_serve, acc, *sums = down_step(
            *(source, blk, gathered[c], acc, down[i], down_serve),
            *(lo, count, skip, n_local, last),
        )
    shared_down_serve = stack_rows(blk, shared_down, acc)
    sums = [acc, *sums]
    total = sums[0]
    for s in range(1, n):
        total = total + give_back(sums[s], "fs", n, s).astype(jnp.float32)
    return (
        total.astype(bf),
        gate_serve,
        up_serve,
        down_serve,
        shared_gate_serve,
        shared_up_serve,
        shared_down_serve,
    )


def body(n, *args):
    return layer(n, *args)


def solution(mesh):
    n = mesh.shape["fs"]
    return jax.shard_map(
        functools.partial(body, n),
        mesh=mesh,
        in_specs=(
            P("fs", "tp"),
            P("fs", None),
            P("fs", None),
            P("fs"),
            P(None, "tp", "fs"),
            P(None, "tp", "fs"),
            P(None, "fs", "tp"),
            P("tp", "fs"),
            P("tp", "fs"),
            P("fs", "tp"),
        ),
        out_specs=(
            P("fs", "tp"),
            P("fs", "tp", None),
            P("fs", "tp", None),
            P("fs", None, "tp"),
            P("tp", None),
            P("tp", None),
            P(None, "tp"),
        ),
        check_vma=False,
    )
```

```python
import functools

import jax
import jax.numpy as jnp
from jax import lax
from jax.experimental import pallas as pl
from jax.experimental.pallas import tpu as pltpu
from jax.sharding import PartitionSpec as P


K = 8

norm_eps = 1e-06
routed_scale = 2.5

VMEM_LIMIT = 60 * 1024 * 1024
ANY = pl.BlockSpec(memory_space=pl.ANY)
VMEM = pl.BlockSpec(memory_space=pltpu.VMEM)
SMEM = pl.BlockSpec(memory_space=pltpu.SMEM)


def partner(i, s, n):
    if n & (n - 1) == 0:
        return i ^ s, i ^ s
    return (i + s) % n, (i + n - s) % n


def exchange(x, axis, n, s):
    return lax.ppermute(x, axis, [(i, partner(i, s, n)[0]) for i in range(n)])


def give_back(x, axis, n, s):
    return lax.ppermute(x, axis, [(i, partner(i, s, n)[1]) for i in range(n)])


def gather_z(x):
    parts = lax.axis_size("tp")
    half = parts // 2
    got = [x]
    for s in range(1, half):
        pairs = [(i, 2 * partner(i // 2, s, half)[0] + i % 2) for i in range(parts)]
        got.append(lax.ppermute(x, "tp", pairs))
    return got


def swap_core(pieces):
    parts = lax.axis_size("tp")
    return [lax.ppermute(x, "tp", [(i, i ^ 1) for i in range(parts)]) for x in pieces]


def gathered_from():
    me = lax.axis_index("tp")
    half = lax.axis_size("tp") // 2
    chips = [partner(me >> 1, s, half)[1] for s in range(half)]
    return [2 * z + core for core in (me & 1, 1 - (me & 1)) for z in chips]


def cuts(count):
    marks = [0] + [-(-count * num // 16) for num in (4, 10, 16)]
    return [(lo, hi - lo) for lo, hi in zip(marks, marks[1:]) if hi > lo]


def down_cuts(chunks):
    steps = [(c, *chunks[c]) for c in range(1, len(chunks))]
    lo, count = chunks[0]
    head = count // 2
    return steps + [(0, *part) for part in ((lo, head), (lo + head, count - head)) if part[1]]


TOKEN = jax.ShapeDtypeStruct((8, 128), jnp.float32)


def prep_gu_body(n, idx_ref, gain_ref, *refs):
    gates, ups, outs = refs[:n], refs[n : 2 * n], refs[2 * n + 1 : 3 * n + 1]
    refs[-1][...] = jnp.zeros(TOKEN.shape, TOKEN.dtype)
    gain = gain_ref[...]
    for s in range(n):
        outs[s][0, 0] = (gates[s][0] * gain).astype(jnp.bfloat16)
        outs[s][1, 0] = (ups[s][0] * gain).astype(jnp.bfloat16)


def prep_gu(gate, up, gain, base, lo, count, token):
    n = base.shape[0]
    _, hp, df = gate.shape
    block = lambda s: pl.BlockSpec((1, hp, df), lambda i, idx, s=s: (idx[s] + lo + i, 0, 0))
    return pl.pallas_call(
        functools.partial(prep_gu_body, n),
        grid_spec=pltpu.PrefetchScalarGridSpec(
            num_scalar_prefetch=1,
            grid=(count,),
            in_specs=[pl.BlockSpec((1, df), lambda i, idx: (0, 0))]
            + [block(s) for s in range(n)] * 2
            + [ANY],
            out_specs=[pl.BlockSpec((2, 1, hp, df), lambda i, idx: (0, i, 0, 0))] * n
            + [pl.BlockSpec(TOKEN.shape, lambda i, idx: (0, 0))],
        ),
        out_shape=[jax.ShapeDtypeStruct((2, count, hp, df), jnp.bfloat16)] * n + [TOKEN],
        compiler_params=pltpu.CompilerParams(vmem_limit_bytes=VMEM_LIMIT),
    )(base, gain, *([gate] * n), *([up] * n), token)


def prep_down_body(n, idx_ref, *refs):
    refs[-1][...] = jnp.zeros(TOKEN.shape, TOKEN.dtype)
    for s in range(n):
        refs[n + 1 + s][0] = refs[s][0].astype(jnp.bfloat16)


def prep_down(down, base, lo, count, token):
    n = base.shape[0]
    _, hf, dp = down.shape
    block = lambda s: pl.BlockSpec((1, hf, dp), lambda i, idx, s=s: (idx[s] + lo + i, 0, 0))
    return pl.pallas_call(
        functools.partial(prep_down_body, n),
        grid_spec=pltpu.PrefetchScalarGridSpec(
            num_scalar_prefetch=1,
            grid=(count,),
            in_specs=[block(s) for s in range(n)] + [ANY],
            out_specs=[pl.BlockSpec((1, hf, dp), lambda i, idx: (i, 0, 0))] * n
            + [pl.BlockSpec(TOKEN.shape, lambda i, idx: (0, 0))],
        ),
        out_shape=[jax.ShapeDtypeStruct((count, hf, dp), jnp.bfloat16)] * n + [TOKEN],
        compiler_params=pltpu.CompilerParams(vmem_limit_bytes=VMEM_LIMIT),
    )(base, *([down] * n), token)


def pack_body(n, *refs):
    own = refs[0].shape[0]
    for s in range(n):
        refs[-1][s * own : (s + 1) * own, :] = refs[s][...]


def pack(pieces, token):
    n = len(pieces)
    own, dp = pieces[0].shape
    return pl.pallas_call(
        functools.partial(pack_body, n),
        in_specs=[VMEM] * n + [ANY],
        out_specs=VMEM,
        out_shape=jax.ShapeDtypeStruct((n * own, dp), pieces[0].dtype),
        name="pack_tokens",
    )(*pieces, token)


def route_body(n, parts, n_local, me_ref, from_ref, *refs):
    gathered, tables, (x_ref, w_ref, inv_ref) = refs[:parts], refs[parts : parts + n], refs[parts + n :]
    own = tables[0].shape[1]
    hp = w_ref.shape[1] // n_local
    width = x_ref.shape[0] * x_ref.shape[2]
    for s in range(n):
        at = pl.ds(s * own, own)
        squares = 0.0
        for k in range(parts):
            narrow = gathered[k][at, :]
            x_ref[from_ref[k], at, :] = narrow
            wide = narrow.astype(jnp.float32)
            squares = squares + jnp.sum(wide * wide, axis=1, keepdims=True)
        inv_ref[at, :] = lax.rsqrt(squares / width + norm_eps)
        table = tables[s][...].T
        ids, affinity = table[:, :K].astype(jnp.int32), table[:, K:]
        weight = routed_scale * affinity / jnp.sum(affinity, axis=1, keepdims=True)
        for e in range(n_local):
            hit = ids == me_ref[0] * n_local + e
            here = jnp.sum(jnp.where(hit, weight, 0.0), axis=1, keepdims=True)
            w_ref[at, e * hp : (e + 1) * hp] = jnp.broadcast_to(here, (own, hp))


def route(me, source, gathered, tables, n_local, hp):
    n, parts = len(tables), len(gathered)
    rows, dp = gathered[0].shape
    return pl.pallas_call(
        functools.partial(route_body, n, parts, n_local),
        in_specs=[SMEM] * 2 + [VMEM] * (parts + n),
        out_specs=[VMEM] * 3,
        out_shape=[
            jax.ShapeDtypeStruct((parts, rows, dp), gathered[0].dtype),
            jax.ShapeDtypeStruct((rows, n_local * hp), jnp.float32),
            jax.ShapeDtypeStruct((rows, 1), jnp.float32),
        ],
        compiler_params=pltpu.CompilerParams(vmem_limit_bytes=VMEM_LIMIT),
        name="route",
    )(me, source, *gathered, *tables)


def shared_down_body(n, parts, me_ref, from_ref, *refs):
    gathered, (down_ref, acc_ref) = refs[:parts], refs[parts:]
    lanes = gathered[0].shape[1]
    share = parts // n
    hp = down_ref.shape[0] // share
    acc_ref[...] = jnp.zeros(acc_ref.shape, acc_ref.dtype)
    for k in range(parts):

        @pl.when(from_ref[k] // share == me_ref[0])
        def _(k=k):
            rows = pl.ds(pl.multiple_of((from_ref[k] % share) * hp, hp), hp)
            acc_ref[...] += jnp.dot(
                gathered[k][:, lanes - hp :], down_ref[rows, :], preferred_element_type=jnp.float32
            )


def shared_down_part(n, me, source, gathered, down):
    parts = len(gathered)
    return pl.pallas_call(
        functools.partial(shared_down_body, n, parts),
        in_specs=[SMEM] * 2 + [VMEM] * (parts + 1),
        out_specs=VMEM,
        out_shape=jax.ShapeDtypeStruct((gathered[0].shape[0], down.shape[1]), jnp.float32),
        compiler_params=pltpu.CompilerParams(vmem_limit_bytes=VMEM_LIMIT),
        name="shared_down",
    )(me, source, *gathered, down)


def stack_rows_body(n, blk_ref, *refs):
    own = refs[0].shape[0]
    for s in range(n):
        refs[-1][pl.ds(pl.multiple_of(blk_ref[s] * own, own), own), :] = refs[s][...]


def stack_rows(blk, pieces, token):
    n = len(pieces)
    own, dp = pieces[0].shape
    return pl.pallas_call(
        functools.partial(stack_rows_body, n),
        in_specs=[SMEM] + [VMEM] * n + [ANY],
        out_specs=VMEM,
        out_shape=jax.ShapeDtypeStruct((n * own, dp), pieces[0].dtype),
        name="stack_rows",
    )(blk, *pieces, token)


def gu_body(n, lo, count, shared, first, *refs):
    refs = list(refs)
    take = lambda k: [refs.pop(0) for _ in range(k)]
    (blk_ref, x_ref, inv_ref, w_ref) = take(4)
    pieces = take(n)
    shared_pieces = take(n) if shared else []
    take(1 if first else 2)
    gate_out, up_out = take(2)
    shared_out = take(2) if shared else []
    (a_ref,) = take(1)
    buf, acc_g, acc_u, in_sem, out_sem = refs
    tot = count + (1 if shared else 0)
    hp, df = buf.shape[-2:]
    dp = x_ref.shape[-1]
    ratio = df // dp
    incoming = []
    for s in range(n):
        here = [pltpu.make_async_copy(pieces[s], buf.at[s, :, pl.ds(0, count)], in_sem.at[s, 0])]
        if shared:
            here.append(
                pltpu.make_async_copy(shared_pieces[s], buf.at[s, :, count], in_sem.at[s, 1])
            )
        for copy in here:
            copy.start()
        incoming.append(here)
    outgoing = []
    nt = (((1,), (1,)), ((), ()))
    for s in range(n):
        for copy in incoming[s]:
            copy.wait()
        blk = blk_ref[s]
        cols = pl.ds(pl.multiple_of(blk * df, df), df)
        here = []
        for m, out in enumerate((gate_out, up_out)):
            here.append(
                pltpu.make_async_copy(
                    buf.at[s, m, pl.ds(0, count)],
                    out.at[pl.ds(lo, count), :, cols],
                    out_sem.at[s, m, 0],
                )
            )
        for m, out in enumerate(shared_out):
            here.append(
                pltpu.make_async_copy(buf.at[s, m, count], out.at[:, cols], out_sem.at[s, m, 1])
            )
        for copy in here:
            copy.start()
        outgoing += here
        for m, acc in enumerate((acc_g, acc_u)):
            part = None
            for j in range(ratio):
                w = buf[s, m, :, :, j * dp : (j + 1) * dp].reshape(tot * hp, dp)
                dot = lax.dot_general(
                    x_ref[blk * ratio + j], w, nt, preferred_element_type=jnp.float32
                )
                part = dot if part is None else part + dot
            if s == 0:
                acc[...] = part
            else:
                acc[...] += part
    inv = inv_ref[...]
    routed = count * hp
    for lanes in [slice(0, routed)] + ([slice(routed, routed + hp)] if shared else []):
        gate = acc_g[:, lanes] * inv
        up = acc_u[:, lanes] * inv
        hidden = gate * jax.nn.sigmoid(gate) * up
        if lanes.start == 0:
            w = w_ref[:, lo * hp : lo * hp + routed]
            hidden = jnp.where(w > 0, hidden * w, 0.0)
        a_ref[:, lanes] = hidden.astype(jnp.bfloat16)
    for copy in outgoing:
        copy.wait()


def gu_step(blk, x, inv, w, pieces, shared_pieces, prev, token, lo, count, n_local, width):
    n = len(pieces)
    hp, df = pieces[0].shape[-2:]
    rows = x.shape[1]
    shared = bool(shared_pieces)
    tot = count + (1 if shared else 0)
    bf = jnp.bfloat16
    out_shape = [jax.ShapeDtypeStruct((n_local, hp, width), bf)] * 2
    if shared:
        out_shape += [jax.ShapeDtypeStruct((hp, width), bf)] * 2
    out_shape.append(jax.ShapeDtypeStruct((rows, tot * hp), bf))
    args = [blk, x, inv, w, *pieces, *shared_pieces, *(prev or [token])]
    specs = [SMEM, VMEM, VMEM, VMEM] + [ANY] * (len(args) - 4)
    aliases = {len(args) - 2: 0, len(args) - 1: 1} if prev else {}
    return pl.pallas_call(
        functools.partial(gu_body, n, lo, count, shared, not prev),
        in_specs=specs,
        out_specs=[ANY] * (len(out_shape) - 1) + [VMEM],
        out_shape=out_shape,
        scratch_shapes=[
            pltpu.VMEM((n, 2, tot, hp, df), bf),
            pltpu.VMEM((rows, tot * hp), jnp.float32),
            pltpu.VMEM((rows, tot * hp), jnp.float32),
            pltpu.SemaphoreType.DMA((n, 2)),
            pltpu.SemaphoreType.DMA((n, 2, 2)),
        ],
        input_output_aliases=aliases,
        compiler_params=pltpu.CompilerParams(vmem_limit_bytes=VMEM_LIMIT),
    )(*args)


def down_body(n, parts, lo, count, skip, first, last, *refs):
    refs = list(refs)
    take = lambda k: [refs.pop(0) for _ in range(k)]
    from_ref, blk_ref = take(2)
    gathered = take(parts)
    (acc_in,) = take(1)
    pieces = take(n)
    if not first:
        take(1)
    (down_out,) = take(1)
    results = take(n) if last else take(1)
    buf, a_buf, acc, in_sem, a_sem, out_sem = refs
    share = parts // n
    _, _, hp, dp = buf.shape
    lanes = count * hp
    copies = []
    for s in range(n):
        for j in range(share):
            part = blk_ref[s] * share + j
            rows = pieces[s].at[:, pl.ds(j * hp, hp), :]
            copies.append(pltpu.make_async_copy(rows, buf.at[part], in_sem.at[s, j]))
    for k in range(parts):
        source = gathered[k].at[:, pl.ds(skip * hp, lanes)]
        copies.append(pltpu.make_async_copy(source, a_buf.at[from_ref[k]], a_sem.at[k]))
    copies.append(pltpu.make_async_copy(acc_in, acc, a_sem.at[parts]))
    for copy in copies:
        copy.start()
    for copy in copies:
        copy.wait()
    out = []
    for p in range(parts):
        rows = down_out.at[pl.ds(lo, count), pl.ds(p * hp, hp), :]
        out.append(pltpu.make_async_copy(buf.at[p], rows, out_sem.at[p]))
    for copy in out:
        copy.start()
    left = jnp.concatenate([a_buf[p] for p in range(parts)], axis=1)
    right = buf[...].reshape(parts * lanes, dp)
    total = acc[...] + jnp.dot(left, right, preferred_element_type=jnp.float32)
    own = acc.shape[0] // n
    if last:
        for r in range(n):
            results[r][...] = total[r * own : (r + 1) * own].astype(results[r].dtype)
    else:
        results[0][...] = total
    for copy in out:
        copy.wait()


def down_body_narrow(n, parts, lo, count, skip, first, last, *refs):
    refs = list(refs)
    take = lambda k: [refs.pop(0) for _ in range(k)]
    from_ref, blk_ref = take(2)
    gathered = take(parts)
    (acc_in,) = take(1)
    pieces = take(n)
    if not first:
        take(1)
    (down_out,) = take(1)
    results = take(n) if last else take(1)
    buf, in_sem, out_sem = refs
    hf = pieces[0].shape[1]
    copies = []
    for s in range(n):
        rows = pl.ds(pl.multiple_of(blk_ref[s] * hf, hf), hf)
        copies.append(pltpu.make_async_copy(pieces[s], buf.at[:, rows], in_sem.at[s]))
    for copy in copies:
        copy.start()
    for copy in copies:
        copy.wait()
    out = pltpu.make_async_copy(buf, down_out.at[pl.ds(lo, count)], out_sem)
    out.start()
    hp = buf.shape[1] // parts
    dp = buf.shape[2]
    lanes = slice(skip * hp, (skip + count) * hp)
    own = acc_in.shape[0] // n
    for r in range(n):
        at = pl.ds(r * own, own)
        total = acc_in[at, :]
        for k in range(parts):
            hidden = pl.ds(pl.multiple_of(from_ref[k] * hp, hp), hp)
            w = buf[:, hidden, :].reshape(count * hp, dp)
            total += jnp.dot(gathered[k][at, lanes], w, preferred_element_type=jnp.float32)
        if last:
            results[r][...] = total.astype(results[r].dtype)
        else:
            results[0][at, :] = total
    out.wait()


def down_step(source, blk, gathered, acc, pieces, prev, lo, count, skip, n_local, last):
    n, parts = len(pieces), len(gathered)
    _, hf, dp = pieces[0].shape
    rows = acc.shape[0]
    own = rows // n
    hidden = hf * n
    hp = hidden // parts
    share = parts // n
    first = prev is None
    bf = jnp.bfloat16
    out_shape = [jax.ShapeDtypeStruct((n_local, hidden, dp), bf)]
    if last:
        out_shape.append(jax.ShapeDtypeStruct((own, dp), jnp.float32))
        out_shape += [jax.ShapeDtypeStruct((own, dp), bf)] * (n - 1)
    else:
        out_shape.append(jax.ShapeDtypeStruct((rows, dp), jnp.float32))
    args = [source, blk, *gathered, acc, *pieces] + ([] if first else [prev])
    specs = [SMEM] * 2 + [ANY] * (len(args) - 2)
    if count * hp % 128 == 0 and skip * hp % 128 == 0 and share * hp == hf:
        kernel = down_body
        scratch = [
            pltpu.VMEM((parts, count, hp, dp), bf),
            pltpu.VMEM((parts, rows, count * hp), bf),
            pltpu.VMEM((rows, dp), jnp.float32),
            pltpu.SemaphoreType.DMA((n, share)),
            pltpu.SemaphoreType.DMA((parts + 1,)),
            pltpu.SemaphoreType.DMA((parts,)),
        ]
    else:
        kernel = down_body_narrow
        specs[2 : parts + 3] = [VMEM] * (parts + 1)
        scratch = [
            pltpu.VMEM((count, hidden, dp), bf),
            pltpu.SemaphoreType.DMA((n,)),
            pltpu.SemaphoreType.DMA,
        ]
    return pl.pallas_call(
        functools.partial(kernel, n, parts, lo, count, skip, first, last),
        in_specs=specs,
        out_specs=[ANY] + [VMEM] * (len(out_shape) - 1),
        out_shape=out_shape,
        scratch_shapes=scratch,
        input_output_aliases={} if first else {len(args) - 1: 0},
        compiler_params=pltpu.CompilerParams(vmem_limit_bytes=VMEM_LIMIT),
    )(*args)


def layer(
    n,
    tokens,
    expert_ids,
    affinity,
    norm_gain,
    gate_train,
    up_train,
    down_train,
    shared_gate_train,
    shared_up_train,
    shared_down_train,
):
    bf = jnp.bfloat16
    me = lax.axis_index("fs")
    experts, hp, _ = gate_train.shape
    n_local = experts // n
    width = norm_gain.shape[0] * n
    to = [partner(me, s, n)[0] for s in range(n)]
    blk = jnp.stack([partner(me, s, n)[1] for s in range(n)]).astype(jnp.int32)
    base = (jnp.stack(to) * n_local).astype(jnp.int32)
    gain = norm_gain[None, :]

    def swap(pieces):
        return [pieces[0]] + [exchange(pieces[s], "fs", n, s) for s in range(1, n)]

    token_pieces = swap([tokens] * n)

    shared_gu = (jnp.stack([shared_gate_train, shared_up_train]) * gain).astype(bf)
    shared_gu = swap([shared_gu] * n)
    table = jnp.concatenate([expert_ids.astype(jnp.float32).T, affinity.T])
    tables = swap([table] * n)
    chunks = cuts(n_local)
    steps = down_cuts(chunks)
    token = tokens
    gu, down = {}, {}
    for c, (lo, count) in enumerate(chunks):
        *pieces, token = prep_gu(gate_train, up_train, gain, base, lo, count, token)
        gu[c] = swap(pieces)
        if c == 0:
            token = packed = pack(token_pieces, token)
            x_same = gather_z(packed)
    for i, (_, lo, count) in enumerate(steps):
        *pieces, token = prep_down(down_train, base, lo, count, token)
        down[i] = swap(pieces)
        if i == 0:
            first_token = token
    own_shared_down = shared_down_train.astype(bf)
    shared_down = swap([own_shared_down] * n)

    x_all = x_same + swap_core(x_same)
    me = me.astype(jnp.int32)[None]
    source = jnp.stack(gathered_from()).astype(jnp.int32)
    x, w, inv = route(me, source, x_all, tables, n_local, hp)
    prev, gathered = [], []
    for c, (lo, count) in enumerate(chunks):
        results = gu_step(
            *(blk, x, inv, w, gu[c], shared_gu if c == 0 else []),
            *(prev, first_token, lo, count, n_local, width),
        )
        if c == 0:
            shared_gate_serve, shared_up_serve = results[2:4]
        prev = results[:2]
        same = gather_z(results[-1])
        gathered.append(same + swap_core(same))
    gate_serve, up_serve = prev

    acc = shared_down_part(n, me, source, gathered[0], own_shared_down)
    down_serve = None
    for i, (c, lo, count) in enumerate(steps):
        last = i == len(steps) - 1
        skip = lo - chunks[c][0]
        down_serve, acc, *sums = down_step(
            *(source, blk, gathered[c], acc, down[i], down_serve),
            *(lo, count, skip, n_local, last),
        )
    shared_down_serve = stack_rows(blk, shared_down, acc)
    sums = [acc, *sums]
    total = sums[0]
    for s in range(1, n):
        total = total + give_back(sums[s], "fs", n, s).astype(jnp.float32)
    return (
        total.astype(bf),
        gate_serve,
        up_serve,
        down_serve,
        shared_gate_serve,
        shared_up_serve,
        shared_down_serve,
    )


def body(n, *args):
    return layer(n, *args)


def solution(mesh):
    n = mesh.shape["fs"]
    return jax.shard_map(
        functools.partial(body, n),
        mesh=mesh,
        in_specs=(
            P("fs", "tp"),
            P("fs", None),
            P("fs", None),
            P("fs"),
            P(None, "tp", "fs"),
            P(None, "tp", "fs"),
            P(None, "fs", "tp"),
            P("tp", "fs"),
            P("tp", "fs"),
            P("fs", "tp"),
        ),
        out_specs=(
            P("fs", "tp"),
            P("fs", "tp", None),
            P("fs", "tp", None),
            P("fs", None, "tp"),
            P("tp", None),
            P("tp", None),
            P(None, "tp"),
        ),
        check_vma=False,
    )
```

```python
import functools

import jax
import jax.numpy as jnp
from jax import lax
from jax.experimental import pallas as pl
from jax.experimental.pallas import tpu as pltpu
from jax.sharding import PartitionSpec as P


K = 8

norm_eps = 1e-06
routed_scale = 2.5

VMEM_LIMIT = 60 * 1024 * 1024
ANY = pl.BlockSpec(memory_space=pl.ANY)
VMEM = pl.BlockSpec(memory_space=pltpu.VMEM)
SMEM = pl.BlockSpec(memory_space=pltpu.SMEM)


def partner(i, s, n):
    if n & (n - 1) == 0:
        return i ^ s, i ^ s
    return (i + s) % n, (i + n - s) % n


def exchange(x, axis, n, s):
    return lax.ppermute(x, axis, [(i, partner(i, s, n)[0]) for i in range(n)])


def give_back(x, axis, n, s):
    return lax.ppermute(x, axis, [(i, partner(i, s, n)[1]) for i in range(n)])


def gather_z(x):
    parts = lax.axis_size("tp")
    half = parts // 2
    got = [x]
    for s in range(1, half):
        pairs = [(i, 2 * partner(i // 2, s, half)[0] + i % 2) for i in range(parts)]
        got.append(lax.ppermute(x, "tp", pairs))
    return got


def swap_core(pieces):
    parts = lax.axis_size("tp")
    return [lax.ppermute(x, "tp", [(i, i ^ 1) for i in range(parts)]) for x in pieces]


def gathered_from():
    me = lax.axis_index("tp")
    half = lax.axis_size("tp") // 2
    chips = [partner(me >> 1, s, half)[1] for s in range(half)]
    return [2 * z + core for core in (me & 1, 1 - (me & 1)) for z in chips]


def cuts(count):
    marks = [0] + [-(-count * num // 16) for num in (2, 8, 16)]
    return [(lo, hi - lo) for lo, hi in zip(marks, marks[1:]) if hi > lo]


def down_cuts(chunks):
    return [(c, *chunks[c]) for c in [*range(1, len(chunks)), 0]]


TOKEN = jax.ShapeDtypeStruct((8, 128), jnp.float32)


def prep_gu_body(n, idx_ref, gain_ref, *refs):
    gates, ups, outs = refs[:n], refs[n : 2 * n], refs[2 * n + 1 : 3 * n + 1]
    refs[-1][...] = jnp.zeros(TOKEN.shape, TOKEN.dtype)
    gain = gain_ref[...]
    for s in range(n):
        outs[s][0, 0] = (gates[s][0] * gain).astype(jnp.bfloat16)
        outs[s][1, 0] = (ups[s][0] * gain).astype(jnp.bfloat16)


def prep_gu(gate, up, gain, base, lo, count, token):
    n = base.shape[0]
    _, hp, df = gate.shape
    block = lambda s: pl.BlockSpec((1, hp, df), lambda i, idx, s=s: (idx[s] + lo + i, 0, 0))
    return pl.pallas_call(
        functools.partial(prep_gu_body, n),
        grid_spec=pltpu.PrefetchScalarGridSpec(
            num_scalar_prefetch=1,
            grid=(count,),
            in_specs=[pl.BlockSpec((1, df), lambda i, idx: (0, 0))]
            + [block(s) for s in range(n)] * 2
            + [ANY],
            out_specs=[pl.BlockSpec((2, 1, hp, df), lambda i, idx: (0, i, 0, 0))] * n
            + [pl.BlockSpec(TOKEN.shape, lambda i, idx: (0, 0))],
        ),
        out_shape=[jax.ShapeDtypeStruct((2, count, hp, df), jnp.bfloat16)] * n + [TOKEN],
        compiler_params=pltpu.CompilerParams(vmem_limit_bytes=VMEM_LIMIT),
    )(base, gain, *([gate] * n), *([up] * n), token)


def prep_down_body(n, idx_ref, *refs):
    refs[-1][...] = jnp.zeros(TOKEN.shape, TOKEN.dtype)
    for s in range(n):
        refs[n + 1 + s][0] = refs[s][0].astype(jnp.bfloat16)


def prep_down(down, base, lo, count, token):
    n = base.shape[0]
    _, hf, dp = down.shape
    block = lambda s: pl.BlockSpec((1, hf, dp), lambda i, idx, s=s: (idx[s] + lo + i, 0, 0))
    return pl.pallas_call(
        functools.partial(prep_down_body, n),
        grid_spec=pltpu.PrefetchScalarGridSpec(
            num_scalar_prefetch=1,
            grid=(count,),
            in_specs=[block(s) for s in range(n)] + [ANY],
            out_specs=[pl.BlockSpec((1, hf, dp), lambda i, idx: (i, 0, 0))] * n
            + [pl.BlockSpec(TOKEN.shape, lambda i, idx: (0, 0))],
        ),
        out_shape=[jax.ShapeDtypeStruct((count, hf, dp), jnp.bfloat16)] * n + [TOKEN],
        compiler_params=pltpu.CompilerParams(vmem_limit_bytes=VMEM_LIMIT),
    )(base, *([down] * n), token)


def pack_body(n, *refs):
    own = refs[0].shape[0]
    for s in range(n):
        refs[-1][s * own : (s + 1) * own, :] = refs[s][...]


def pack(pieces, token):
    n = len(pieces)
    own, dp = pieces[0].shape
    return pl.pallas_call(
        functools.partial(pack_body, n),
        in_specs=[VMEM] * n + [ANY],
        out_specs=VMEM,
        out_shape=jax.ShapeDtypeStruct((n * own, dp), pieces[0].dtype),
        name="pack_tokens",
    )(*pieces, token)


def route_body(n, parts, n_local, me_ref, from_ref, *refs):
    gathered, tables, (x_ref, w_ref, inv_ref) = refs[:parts], refs[parts : parts + n], refs[parts + n :]
    own = tables[0].shape[1]
    hp = w_ref.shape[1] // n_local
    width = x_ref.shape[0] * x_ref.shape[2]
    for s in range(n):
        at = pl.ds(s * own, own)
        squares = 0.0
        for k in range(parts):
            narrow = gathered[k][at, :]
            x_ref[from_ref[k], at, :] = narrow
            wide = narrow.astype(jnp.float32)
            squares = squares + jnp.sum(wide * wide, axis=1, keepdims=True)
        inv_ref[at, :] = lax.rsqrt(squares / width + norm_eps)
        table = tables[s][...].T
        ids, affinity = table[:, :K].astype(jnp.int32), table[:, K:]
        weight = routed_scale * affinity / jnp.sum(affinity, axis=1, keepdims=True)
        for e in range(n_local):
            hit = ids == me_ref[0] * n_local + e
            here = jnp.sum(jnp.where(hit, weight, 0.0), axis=1, keepdims=True)
            w_ref[at, e * hp : (e + 1) * hp] = jnp.broadcast_to(here, (own, hp))


def route(me, source, gathered, tables, n_local, hp):
    n, parts = len(tables), len(gathered)
    rows, dp = gathered[0].shape
    return pl.pallas_call(
        functools.partial(route_body, n, parts, n_local),
        in_specs=[SMEM] * 2 + [VMEM] * (parts + n),
        out_specs=[VMEM] * 3,
        out_shape=[
            jax.ShapeDtypeStruct((parts, rows, dp), gathered[0].dtype),
            jax.ShapeDtypeStruct((rows, n_local * hp), jnp.float32),
            jax.ShapeDtypeStruct((rows, 1), jnp.float32),
        ],
        compiler_params=pltpu.CompilerParams(vmem_limit_bytes=VMEM_LIMIT),
        name="route",
    )(me, source, *gathered, *tables)


def shared_down_body(n, parts, me_ref, from_ref, *refs):
    gathered, (down_ref, acc_ref) = refs[:parts], refs[parts:]
    lanes = gathered[0].shape[1]
    share = parts // n
    hp = down_ref.shape[0] // share
    acc_ref[...] = jnp.zeros(acc_ref.shape, acc_ref.dtype)
    for k in range(parts):

        @pl.when(from_ref[k] // share == me_ref[0])
        def _(k=k):
            rows = pl.ds(pl.multiple_of((from_ref[k] % share) * hp, hp), hp)
            acc_ref[...] += jnp.dot(
                gathered[k][:, lanes - hp :], down_ref[rows, :], preferred_element_type=jnp.float32
            )


def shared_down_part(n, me, source, gathered, down):
    parts = len(gathered)
    return pl.pallas_call(
        functools.partial(shared_down_body, n, parts),
        in_specs=[SMEM] * 2 + [VMEM] * (parts + 1),
        out_specs=VMEM,
        out_shape=jax.ShapeDtypeStruct((gathered[0].shape[0], down.shape[1]), jnp.float32),
        compiler_params=pltpu.CompilerParams(vmem_limit_bytes=VMEM_LIMIT),
        name="shared_down",
    )(me, source, *gathered, down)


def finish_body(n, lo, count, blk_ref, *refs):
    pieces, shared_pieces, refs = refs[:n], refs[n : 2 * n], refs[2 * n + 2 :]
    down_out, shared_out, buf, in_sem, out_sem = refs
    hf = pieces[0].shape[1]
    copies = []
    for s in range(n):
        rows = pl.ds(pl.multiple_of(blk_ref[s] * hf, hf), hf)
        head = buf.at[pl.ds(0, count), rows]
        copies.append(pltpu.make_async_copy(pieces[s], head, in_sem.at[s, 0]))
        copies.append(pltpu.make_async_copy(shared_pieces[s], buf.at[count, rows], in_sem.at[s, 1]))
    for copy in copies:
        copy.start()
    for copy in copies:
        copy.wait()
    copies = [
        pltpu.make_async_copy(
            buf.at[pl.ds(0, count)], down_out.at[pl.ds(lo, count)], out_sem.at[0]
        ),
        pltpu.make_async_copy(buf.at[count], shared_out, out_sem.at[1]),
    ]
    for copy in copies:
        copy.start()
    for copy in copies:
        copy.wait()


def finish(blk, pieces, shared_pieces, down_serve, token, lo):
    n = len(pieces)
    count, hf, dp = pieces[0].shape
    return pl.pallas_call(
        functools.partial(finish_body, n, lo, count),
        in_specs=[SMEM] + [ANY] * (2 * n + 2),
        out_specs=[ANY] * 2,
        out_shape=[
            jax.ShapeDtypeStruct(down_serve.shape, down_serve.dtype),
            jax.ShapeDtypeStruct((n * hf, dp), down_serve.dtype),
        ],
        scratch_shapes=[
            pltpu.VMEM((count + 1, n * hf, dp), down_serve.dtype),
            pltpu.SemaphoreType.DMA((n, 2)),
            pltpu.SemaphoreType.DMA((2,)),
        ],
        input_output_aliases={2 * n + 2: 0},
        name="finish",
    )(blk, *pieces, *shared_pieces, token, down_serve)


def gu_body(n, lo, count, shared, first, *refs):
    refs = list(refs)
    take = lambda k: [refs.pop(0) for _ in range(k)]
    (blk_ref, x_ref, inv_ref, w_ref) = take(4)
    pieces = take(n)
    shared_pieces = [take(k) for k in shared]
    take(1 if first else 2)
    gate_out, up_out = take(2)
    shared_out = take(2) if shared else []
    (a_ref,) = take(1)
    buf, acc_g, acc_u, in_sem, out_sem = refs
    tot = count + (1 if shared else 0)
    hp, df = buf.shape[-2:]
    dp = x_ref.shape[-1]
    ratio = df // dp
    incoming = []
    for s in range(n):
        here = [pltpu.make_async_copy(pieces[s], buf.at[s, :, pl.ds(0, count)], in_sem.at[s, 0])]
        if shared and shared[s] == 1:
            whole = shared_pieces[s][0]
            here.append(pltpu.make_async_copy(whole, buf.at[s, :, count], in_sem.at[s, 1]))
        elif shared:
            for m in range(2):
                part = shared_pieces[s][m]
                here.append(
                    pltpu.make_async_copy(part, buf.at[s, m, count], in_sem.at[s, 1 + m])
                )
        for copy in here:
            copy.start()
        incoming.append(here)
    outgoing = []
    nt = (((1,), (1,)), ((), ()))
    for s in range(n):
        for copy in incoming[s]:
            copy.wait()
        blk = blk_ref[s]
        cols = pl.ds(pl.multiple_of(blk * df, df), df)
        here = []
        for m, out in enumerate((gate_out, up_out)):
            here.append(
                pltpu.make_async_copy(
                    buf.at[s, m, pl.ds(0, count)],
                    out.at[pl.ds(lo, count), :, cols],
                    out_sem.at[s, m, 0],
                )
            )
        for m, out in enumerate(shared_out):
            here.append(
                pltpu.make_async_copy(buf.at[s, m, count], out.at[:, cols], out_sem.at[s, m, 1])
            )
        for copy in here:
            copy.start()
        outgoing += here
        for m, acc in enumerate((acc_g, acc_u)):
            part = None
            for j in range(ratio):
                w = buf[s, m, :, :, j * dp : (j + 1) * dp].reshape(tot * hp, dp)
                dot = lax.dot_general(
                    x_ref[blk * ratio + j], w, nt, preferred_element_type=jnp.float32
                )
                part = dot if part is None else part + dot
            if s == 0:
                acc[...] = part
            else:
                acc[...] += part
    inv = inv_ref[...]
    routed = count * hp
    for lanes in [slice(0, routed)] + ([slice(routed, routed + hp)] if shared else []):
        gate = acc_g[:, lanes] * inv
        up = acc_u[:, lanes] * inv
        hidden = gate * jax.nn.sigmoid(gate) * up
        if lanes.start == 0:
            w = w_ref[:, lo * hp : lo * hp + routed]
            hidden = jnp.where(w > 0, hidden * w, 0.0)
        a_ref[:, lanes] = hidden.astype(jnp.bfloat16)
    for copy in outgoing:
        copy.wait()


def gu_step(blk, x, inv, w, pieces, shared_pieces, prev, token, lo, count, n_local, width):
    n = len(pieces)
    hp, df = pieces[0].shape[-2:]
    rows = x.shape[1]
    shared = tuple(len(group) for group in shared_pieces)
    shared_pieces = [piece for group in shared_pieces for piece in group]
    tot = count + (1 if shared else 0)
    bf = jnp.bfloat16
    out_shape = [jax.ShapeDtypeStruct((n_local, hp, width), bf)] * 2
    if shared:
        out_shape += [jax.ShapeDtypeStruct((hp, width), bf)] * 2
    out_shape.append(jax.ShapeDtypeStruct((rows, tot * hp), bf))
    args = [blk, x, inv, w, *pieces, *shared_pieces, *(prev or [token])]
    specs = [SMEM, VMEM, VMEM, VMEM] + [ANY] * (len(args) - 4)
    aliases = {len(args) - 2: 0, len(args) - 1: 1} if prev else {}
    return pl.pallas_call(
        functools.partial(gu_body, n, lo, count, shared, not prev),
        in_specs=specs,
        out_specs=[ANY] * (len(out_shape) - 1) + [VMEM],
        out_shape=out_shape,
        scratch_shapes=[
            pltpu.VMEM((n, 2, tot, hp, df), bf),
            pltpu.VMEM((rows, tot * hp), jnp.float32),
            pltpu.VMEM((rows, tot * hp), jnp.float32),
            pltpu.SemaphoreType.DMA((n, 3)),
            pltpu.SemaphoreType.DMA((n, 2, 2)),
        ],
        input_output_aliases=aliases,
        compiler_params=pltpu.CompilerParams(vmem_limit_bytes=VMEM_LIMIT),
    )(*args)


def down_body(n, parts, lo, count, skip, first, last, *refs):
    refs = list(refs)
    take = lambda k: [refs.pop(0) for _ in range(k)]
    from_ref, blk_ref = take(2)
    gathered = take(parts)
    (acc_in,) = take(1)
    pieces = take(n)
    if not first and not last:
        take(1)
    (down_out,) = [None] if last else take(1)
    results = take(n) if last else take(1)
    buf, a_buf, acc, in_sem, a_sem, out_sem = refs
    share = parts // n
    _, _, hp, dp = buf.shape
    lanes = count * hp
    copies = []
    for s in range(n):
        for j in range(share):
            part = blk_ref[s] * share + j
            rows = pieces[s].at[:, pl.ds(j * hp, hp), :]
            copies.append(pltpu.make_async_copy(rows, buf.at[part], in_sem.at[s, j]))
    for k in range(parts):
        source = gathered[k].at[:, pl.ds(skip * hp, lanes)]
        copies.append(pltpu.make_async_copy(source, a_buf.at[from_ref[k]], a_sem.at[k]))
    copies.append(pltpu.make_async_copy(acc_in, acc, a_sem.at[parts]))
    for copy in copies:
        copy.start()
    for copy in copies:
        copy.wait()
    out = []
    for p in range(0 if last else parts):
        rows = down_out.at[pl.ds(lo, count), pl.ds(p * hp, hp), :]
        out.append(pltpu.make_async_copy(buf.at[p], rows, out_sem.at[p]))
    for copy in out:
        copy.start()
    left = jnp.concatenate([a_buf[p] for p in range(parts)], axis=1)
    right = buf[...].reshape(parts * lanes, dp)
    total = acc[...] + jnp.dot(left, right, preferred_element_type=jnp.float32)
    own = acc.shape[0] // n
    if last:
        for r in range(n):
            results[r][...] = total[r * own : (r + 1) * own].astype(results[r].dtype)
    else:
        results[0][...] = total
    for copy in out:
        copy.wait()


def down_body_narrow(n, parts, lo, count, skip, first, last, *refs):
    refs = list(refs)
    take = lambda k: [refs.pop(0) for _ in range(k)]
    from_ref, blk_ref = take(2)
    gathered = take(parts)
    (acc_in,) = take(1)
    pieces = take(n)
    if not first and not last:
        take(1)
    (down_out,) = [None] if last else take(1)
    results = take(n) if last else take(1)
    buf, in_sem, out_sem = refs
    hf = pieces[0].shape[1]
    copies = []
    for s in range(n):
        rows = pl.ds(pl.multiple_of(blk_ref[s] * hf, hf), hf)
        copies.append(pltpu.make_async_copy(pieces[s], buf.at[:, rows], in_sem.at[s]))
    for copy in copies:
        copy.start()
    for copy in copies:
        copy.wait()
    if not last:
        out = pltpu.make_async_copy(buf, down_out.at[pl.ds(lo, count)], out_sem)
        out.start()
    hp = buf.shape[1] // parts
    dp = buf.shape[2]
    lanes = slice(skip * hp, (skip + count) * hp)
    own = acc_in.shape[0] // n
    for r in range(n):
        at = pl.ds(r * own, own)
        total = acc_in[at, :]
        for k in range(parts):
            hidden = pl.ds(pl.multiple_of(from_ref[k] * hp, hp), hp)
            w = buf[:, hidden, :].reshape(count * hp, dp)
            total += jnp.dot(gathered[k][at, lanes], w, preferred_element_type=jnp.float32)
        if last:
            results[r][...] = total.astype(results[r].dtype)
        else:
            results[0][at, :] = total
    if not last:
        out.wait()


def down_step(source, blk, gathered, acc, pieces, prev, lo, count, skip, n_local, last):
    n, parts = len(pieces), len(gathered)
    _, hf, dp = pieces[0].shape
    rows = acc.shape[0]
    own = rows // n
    hidden = hf * n
    hp = hidden // parts
    share = parts // n
    first = prev is None
    bf = jnp.bfloat16
    if last:
        out_shape = [jax.ShapeDtypeStruct((own, dp), jnp.float32)]
        out_shape += [jax.ShapeDtypeStruct((own, dp), bf)] * (n - 1)
    else:
        out_shape = [jax.ShapeDtypeStruct((n_local, hidden, dp), bf)]
        out_shape.append(jax.ShapeDtypeStruct((rows, dp), jnp.float32))
    args = [source, blk, *gathered, acc, *pieces] + ([] if first or last else [prev])
    specs = [SMEM] * 2 + [ANY] * (len(args) - 2)
    if count * hp % 128 == 0 and skip * hp % 128 == 0 and share * hp == hf:
        kernel = down_body
        scratch = [
            pltpu.VMEM((parts, count, hp, dp), bf),
            pltpu.VMEM((parts, rows, count * hp), bf),
            pltpu.VMEM((rows, dp), jnp.float32),
            pltpu.SemaphoreType.DMA((n, share)),
            pltpu.SemaphoreType.DMA((parts + 1,)),
            pltpu.SemaphoreType.DMA((parts,)),
        ]
    else:
        kernel = down_body_narrow
        specs[2 : parts + 3] = [VMEM] * (parts + 1)
        scratch = [
            pltpu.VMEM((count, hidden, dp), bf),
            pltpu.SemaphoreType.DMA((n,)),
            pltpu.SemaphoreType.DMA,
        ]
    return pl.pallas_call(
        functools.partial(kernel, n, parts, lo, count, skip, first, last),
        in_specs=specs,
        out_specs=[VMEM] * n if last else [ANY, VMEM],
        out_shape=out_shape,
        scratch_shapes=scratch,
        input_output_aliases={} if first or last else {len(args) - 1: 0},
        compiler_params=pltpu.CompilerParams(vmem_limit_bytes=VMEM_LIMIT),
    )(*args)


def layer(
    n,
    tokens,
    expert_ids,
    affinity,
    norm_gain,
    gate_train,
    up_train,
    down_train,
    shared_gate_train,
    shared_up_train,
    shared_down_train,
):
    bf = jnp.bfloat16
    me = lax.axis_index("fs")
    experts, hp, _ = gate_train.shape
    n_local = experts // n
    width = norm_gain.shape[0] * n
    to = [partner(me, s, n)[0] for s in range(n)]
    blk = jnp.stack([partner(me, s, n)[1] for s in range(n)]).astype(jnp.int32)
    base = (jnp.stack(to) * n_local).astype(jnp.int32)
    gain = norm_gain[None, :]

    def swap(pieces):
        return [pieces[0]] + [exchange(pieces[s], "fs", n, s) for s in range(1, n)]

    token_pieces = swap([tokens] * n)

    shared_gu = (jnp.stack([shared_gate_train, shared_up_train]) * gain).astype(bf)
    if n == 4:
        near = [exchange(shared_gu, "fs", n, s) for s in (1, 2)]
        far = [exchange(near[0][0], "fs", n, 2), exchange(near[1][1], "fs", n, 1)]
        shared_gu = [[shared_gu], *([piece] for piece in near), far]
    else:
        shared_gu = [[piece] for piece in swap([shared_gu] * n)]
    table = jnp.concatenate([expert_ids.astype(jnp.float32).T, affinity.T])
    tables = swap([table] * n)
    chunks = cuts(n_local)
    steps = down_cuts(chunks)
    token = tokens
    gu, down = {}, {}
    for c, (lo, count) in enumerate(chunks):
        *pieces, token = prep_gu(gate_train, up_train, gain, base, lo, count, token)
        gu[c] = swap(pieces)
        if c == 1:
            token = packed = pack(token_pieces, token)
            x_same = gather_z(packed)
    for i, (_, lo, count) in enumerate(steps):
        *pieces, token = prep_down(down_train, base, lo, count, token)
        down[i] = swap(pieces)
        if i == len(steps) - 2:
            first_token = token
    own_shared_down = shared_down_train.astype(bf)
    shared_down = swap([own_shared_down] * n)

    x_all = x_same + swap_core(x_same)
    me = me.astype(jnp.int32)[None]
    source = jnp.stack(gathered_from()).astype(jnp.int32)
    x, w, inv = route(me, source, x_all, tables, n_local, hp)
    prev, gathered = [], []
    for c, (lo, count) in enumerate(chunks):
        results = gu_step(
            *(blk, x, inv, w, gu[c], shared_gu if c == 0 else []),
            *(prev, first_token, lo, count, n_local, width),
        )
        if c == 0:
            shared_gate_serve, shared_up_serve = results[2:4]
        prev = results[:2]
        same = gather_z(results[-1])
        gathered.append(same + swap_core(same))
    gate_serve, up_serve = prev

    acc = shared_down_part(n, me, source, gathered[0], own_shared_down)
    down_serve = None
    for i, (c, lo, count) in enumerate(steps):
        last = i == len(steps) - 1
        results = down_step(
            *(source, blk, gathered[c], acc, down[i], down_serve),
            *(lo, count, lo - chunks[c][0], n_local, last),
        )
        if not last:
            down_serve, acc = results
    sums = list(results)
    back = [give_back(sums[s], "fs", n, s) for s in range(1, n)]
    down_serve, shared_down_serve = finish(
        blk, down[len(steps) - 1], shared_down, down_serve, sums[0], steps[-1][1]
    )
    total = sums[0]
    for part in back:
        total = total + part.astype(jnp.float32)
    return (
        total.astype(bf),
        gate_serve,
        up_serve,
        down_serve,
        shared_gate_serve,
        shared_up_serve,
        shared_down_serve,
    )


def body(n, *args):
    return layer(n, *args)


def solution(mesh):
    n = mesh.shape["fs"]
    return jax.shard_map(
        functools.partial(body, n),
        mesh=mesh,
        in_specs=(
            P("fs", "tp"),
            P("fs", None),
            P("fs", None),
            P("fs"),
            P(None, "tp", "fs"),
            P(None, "tp", "fs"),
            P(None, "fs", "tp"),
            P("tp", "fs"),
            P("tp", "fs"),
            P("fs", "tp"),
        ),
        out_specs=(
            P("fs", "tp"),
            P("fs", "tp", None),
            P("fs", "tp", None),
            P("fs", None, "tp"),
            P("tp", None),
            P("tp", None),
            P(None, "tp"),
        ),
        check_vma=False,
    )
```

```python
import functools

import jax
import jax.numpy as jnp
from jax import lax
from jax.experimental import pallas as pl
from jax.experimental.pallas import tpu as pltpu
from jax.sharding import PartitionSpec as P


K = 8

norm_eps = 1e-06
routed_scale = 2.5

VMEM_LIMIT = 60 * 1024 * 1024
ANY = pl.BlockSpec(memory_space=pl.ANY)
VMEM = pl.BlockSpec(memory_space=pltpu.VMEM)
SMEM = pl.BlockSpec(memory_space=pltpu.SMEM)


def partner(i, s, n):
    if n & (n - 1) == 0:
        return i ^ s, i ^ s
    return (i + s) % n, (i + n - s) % n


def exchange(x, axis, n, s):
    return lax.ppermute(x, axis, [(i, partner(i, s, n)[0]) for i in range(n)])


def give_back(x, axis, n, s):
    return lax.ppermute(x, axis, [(i, partner(i, s, n)[1]) for i in range(n)])


def gather_z(x):
    parts = lax.axis_size("tp")
    half = parts // 2
    got = [x]
    for s in range(1, half):
        pairs = [(i, 2 * partner(i // 2, s, half)[0] + i % 2) for i in range(parts)]
        got.append(lax.ppermute(x, "tp", pairs))
    return got


def swap_core(pieces):
    parts = lax.axis_size("tp")
    return [lax.ppermute(x, "tp", [(i, i ^ 1) for i in range(parts)]) for x in pieces]


def gathered_from():
    me = lax.axis_index("tp")
    half = lax.axis_size("tp") // 2
    chips = [partner(me >> 1, s, half)[1] for s in range(half)]
    return [2 * z + core for core in (me & 1, 1 - (me & 1)) for z in chips]


def cuts(count):
    marks = [0] + [-(-count * num // 16) for num in (2, 8, 16)]
    return [(lo, hi - lo) for lo, hi in zip(marks, marks[1:]) if hi > lo]


def down_cuts(chunks):
    return [(c, *chunks[c]) for c in [*range(1, len(chunks)), 0]]


TOKEN = jax.ShapeDtypeStruct((8, 128), jnp.float32)


def prep_gu_body(n, idx_ref, gain_ref, *refs):
    gates, ups, outs = refs[:n], refs[n : 2 * n], refs[2 * n + 1 : 3 * n + 1]
    refs[-1][...] = jnp.zeros(TOKEN.shape, TOKEN.dtype)
    gain = gain_ref[...]
    for s in range(n):
        outs[s][0, 0] = (gates[s][0] * gain).astype(jnp.bfloat16)
        outs[s][1, 0] = (ups[s][0] * gain).astype(jnp.bfloat16)


def prep_gu(gate, up, gain, base, lo, count, token):
    n = base.shape[0]
    _, hp, df = gate.shape
    block = lambda s: pl.BlockSpec((1, hp, df), lambda i, idx, s=s: (idx[s] + lo + i, 0, 0))
    return pl.pallas_call(
        functools.partial(prep_gu_body, n),
        grid_spec=pltpu.PrefetchScalarGridSpec(
            num_scalar_prefetch=1,
            grid=(count,),
            in_specs=[pl.BlockSpec((1, df), lambda i, idx: (0, 0))]
            + [block(s) for s in range(n)] * 2
            + [ANY],
            out_specs=[pl.BlockSpec((2, 1, hp, df), lambda i, idx: (0, i, 0, 0))] * n
            + [pl.BlockSpec(TOKEN.shape, lambda i, idx: (0, 0))],
        ),
        out_shape=[jax.ShapeDtypeStruct((2, count, hp, df), jnp.bfloat16)] * n + [TOKEN],
        compiler_params=pltpu.CompilerParams(vmem_limit_bytes=VMEM_LIMIT),
    )(base, gain, *([gate] * n), *([up] * n), token)


def prep_down_body(n, idx_ref, *refs):
    refs[-1][...] = jnp.zeros(TOKEN.shape, TOKEN.dtype)
    for s in range(n):
        refs[n + 1 + s][0] = refs[s][0].astype(jnp.bfloat16)


def prep_down(down, base, lo, count, token):
    n = base.shape[0]
    _, hf, dp = down.shape
    block = lambda s: pl.BlockSpec((1, hf, dp), lambda i, idx, s=s: (idx[s] + lo + i, 0, 0))
    return pl.pallas_call(
        functools.partial(prep_down_body, n),
        grid_spec=pltpu.PrefetchScalarGridSpec(
            num_scalar_prefetch=1,
            grid=(count,),
            in_specs=[block(s) for s in range(n)] + [ANY],
            out_specs=[pl.BlockSpec((1, hf, dp), lambda i, idx: (i, 0, 0))] * n
            + [pl.BlockSpec(TOKEN.shape, lambda i, idx: (0, 0))],
        ),
        out_shape=[jax.ShapeDtypeStruct((count, hf, dp), jnp.bfloat16)] * n + [TOKEN],
        compiler_params=pltpu.CompilerParams(vmem_limit_bytes=VMEM_LIMIT),
    )(base, *([down] * n), token)


def pack_body(n, *refs):
    own = refs[0].shape[0]
    for s in range(n):
        refs[-1][s * own : (s + 1) * own, :] = refs[s][...]


def pack(pieces, token):
    n = len(pieces)
    own, dp = pieces[0].shape
    return pl.pallas_call(
        functools.partial(pack_body, n),
        in_specs=[VMEM] * n + [ANY],
        out_specs=VMEM,
        out_shape=jax.ShapeDtypeStruct((n * own, dp), pieces[0].dtype),
        name="pack_tokens",
    )(*pieces, token)


def route_body(n, parts, n_local, me_ref, from_ref, *refs):
    gathered, tables, (x_ref, w_ref, inv_ref) = refs[:parts], refs[parts : parts + n], refs[parts + n :]
    own = tables[0].shape[1]
    hp = w_ref.shape[1] // n_local
    width = x_ref.shape[0] * x_ref.shape[2]
    for s in range(n):
        at = pl.ds(s * own, own)
        squares = 0.0
        for k in range(parts):
            narrow = gathered[k][at, :]
            x_ref[from_ref[k], at, :] = narrow
            wide = narrow.astype(jnp.float32)
            squares = squares + jnp.sum(wide * wide, axis=1, keepdims=True)
        inv_ref[at, :] = lax.rsqrt(squares / width + norm_eps)
        table = tables[s][...].T
        ids, affinity = table[:, :K].astype(jnp.int32), table[:, K:]
        weight = routed_scale * affinity / jnp.sum(affinity, axis=1, keepdims=True)
        for e in range(n_local):
            hit = ids == me_ref[0] * n_local + e
            here = jnp.sum(jnp.where(hit, weight, 0.0), axis=1, keepdims=True)
            w_ref[at, e * hp : (e + 1) * hp] = jnp.broadcast_to(here, (own, hp))


def route(me, source, gathered, tables, n_local, hp):
    n, parts = len(tables), len(gathered)
    rows, dp = gathered[0].shape
    return pl.pallas_call(
        functools.partial(route_body, n, parts, n_local),
        in_specs=[SMEM] * 2 + [VMEM] * (parts + n),
        out_specs=[VMEM] * 3,
        out_shape=[
            jax.ShapeDtypeStruct((parts, rows, dp), gathered[0].dtype),
            jax.ShapeDtypeStruct((rows, n_local * hp), jnp.float32),
            jax.ShapeDtypeStruct((rows, 1), jnp.float32),
        ],
        compiler_params=pltpu.CompilerParams(vmem_limit_bytes=VMEM_LIMIT),
        name="route",
    )(me, source, *gathered, *tables)


def shared_down_body(n, parts, me_ref, from_ref, *refs):
    gathered, (down_ref, acc_ref) = refs[:parts], refs[parts:]
    lanes = gathered[0].shape[1]
    share = parts // n
    hp = down_ref.shape[0] // share
    acc_ref[...] = jnp.zeros(acc_ref.shape, acc_ref.dtype)
    for k in range(parts):

        @pl.when(from_ref[k] // share == me_ref[0])
        def _(k=k):
            rows = pl.ds(pl.multiple_of((from_ref[k] % share) * hp, hp), hp)
            acc_ref[...] += jnp.dot(
                gathered[k][:, lanes - hp :], down_ref[rows, :], preferred_element_type=jnp.float32
            )


def shared_down_part(n, me, source, gathered, down):
    parts = len(gathered)
    return pl.pallas_call(
        functools.partial(shared_down_body, n, parts),
        in_specs=[SMEM] * 2 + [VMEM] * (parts + 1),
        out_specs=VMEM,
        out_shape=jax.ShapeDtypeStruct((gathered[0].shape[0], down.shape[1]), jnp.float32),
        compiler_params=pltpu.CompilerParams(vmem_limit_bytes=VMEM_LIMIT),
        name="shared_down",
    )(me, source, *gathered, down)


def finish_body(n, lo, count, blk_ref, *refs):
    pieces, shared_pieces, refs = refs[:n], refs[n : 2 * n], refs[2 * n + 2 :]
    down_out, shared_out, buf, in_sem, out_sem = refs
    hf = pieces[0].shape[1]
    arriving, leaving = [], []
    for s in range(n):
        rows = pl.ds(pl.multiple_of(blk_ref[s] * hf, hf), hf)
        moves = [
            (pieces[s], buf.at[pl.ds(0, count), rows], down_out.at[pl.ds(lo, count), rows]),
            (shared_pieces[s], buf.at[count, rows], shared_out.at[rows]),
        ]
        for m, (source, stage, target) in enumerate(moves):
            arriving.append(pltpu.make_async_copy(source, stage, in_sem.at[s, m]))
            leaving.append(pltpu.make_async_copy(stage, target, out_sem.at[s, m]))
    for copy in arriving:
        copy.start()
    for copy, onward in zip(arriving, leaving):
        copy.wait()
        onward.start()
    for copy in leaving:
        copy.wait()


def finish(blk, pieces, shared_pieces, down_serve, token, lo):
    n = len(pieces)
    count, hf, dp = pieces[0].shape
    return pl.pallas_call(
        functools.partial(finish_body, n, lo, count),
        in_specs=[SMEM] + [ANY] * (2 * n + 2),
        out_specs=[ANY] * 2,
        out_shape=[
            jax.ShapeDtypeStruct(down_serve.shape, down_serve.dtype),
            jax.ShapeDtypeStruct((n * hf, dp), down_serve.dtype),
        ],
        scratch_shapes=[
            pltpu.VMEM((count + 1, n * hf, dp), down_serve.dtype),
            pltpu.SemaphoreType.DMA((n, 2)),
            pltpu.SemaphoreType.DMA((n, 2)),
        ],
        input_output_aliases={2 * n + 2: 0},
        name="finish",
    )(blk, *pieces, *shared_pieces, token, down_serve)


def gu_body(n, lo, count, shared, first, *refs):
    refs = list(refs)
    take = lambda k: [refs.pop(0) for _ in range(k)]
    (blk_ref, x_ref, inv_ref, w_ref) = take(4)
    pieces = take(n)
    shared_pieces = [take(k) for k in shared]
    take(1 if first else 2)
    gate_out, up_out = take(2)
    shared_out = take(2) if shared else []
    (a_ref,) = take(1)
    buf, acc_g, acc_u, in_sem, out_sem = refs
    tot = count + (1 if shared else 0)
    hp, df = buf.shape[-2:]
    dp = x_ref.shape[-1]
    ratio = df // dp
    incoming = []
    for s in range(n):
        here = [pltpu.make_async_copy(pieces[s], buf.at[s, :, pl.ds(0, count)], in_sem.at[s, 0])]
        if shared and shared[s] == 1:
            whole = shared_pieces[s][0]
            here.append(pltpu.make_async_copy(whole, buf.at[s, :, count], in_sem.at[s, 1]))
        elif shared:
            for m in range(2):
                part = shared_pieces[s][m]
                here.append(
                    pltpu.make_async_copy(part, buf.at[s, m, count], in_sem.at[s, 1 + m])
                )
        for copy in here:
            copy.start()
        incoming.append(here)
    outgoing = []
    nt = (((1,), (1,)), ((), ()))
    for s in range(n):
        for copy in incoming[s]:
            copy.wait()
        blk = blk_ref[s]
        cols = pl.ds(pl.multiple_of(blk * df, df), df)
        here = []
        for m, out in enumerate((gate_out, up_out)):
            here.append(
                pltpu.make_async_copy(
                    buf.at[s, m, pl.ds(0, count)],
                    out.at[pl.ds(lo, count), :, cols],
                    out_sem.at[s, m, 0],
                )
            )
        for m, out in enumerate(shared_out):
            here.append(
                pltpu.make_async_copy(buf.at[s, m, count], out.at[:, cols], out_sem.at[s, m, 1])
            )
        for copy in here:
            copy.start()
        outgoing += here
        for m, acc in enumerate((acc_g, acc_u)):
            part = None
            for j in range(ratio):
                w = buf[s, m, :, :, j * dp : (j + 1) * dp].reshape(tot * hp, dp)
                dot = lax.dot_general(
                    x_ref[blk * ratio + j], w, nt, preferred_element_type=jnp.float32
                )
                part = dot if part is None else part + dot
            if s == 0:
                acc[...] = part
            else:
                acc[...] += part
    inv = inv_ref[...]
    routed = count * hp
    for lanes in [slice(0, routed)] + ([slice(routed, routed + hp)] if shared else []):
        gate = acc_g[:, lanes] * inv
        up = acc_u[:, lanes] * inv
        hidden = gate * jax.nn.sigmoid(gate) * up
        if lanes.start == 0:
            w = w_ref[:, lo * hp : lo * hp + routed]
            hidden = jnp.where(w > 0, hidden * w, 0.0)
        a_ref[:, lanes] = hidden.astype(jnp.bfloat16)
    for copy in outgoing:
        copy.wait()


def gu_step(blk, x, inv, w, pieces, shared_pieces, prev, token, lo, count, n_local, width):
    n = len(pieces)
    hp, df = pieces[0].shape[-2:]
    rows = x.shape[1]
    shared = tuple(len(group) for group in shared_pieces)
    shared_pieces = [piece for group in shared_pieces for piece in group]
    tot = count + (1 if shared else 0)
    bf = jnp.bfloat16
    out_shape = [jax.ShapeDtypeStruct((n_local, hp, width), bf)] * 2
    if shared:
        out_shape += [jax.ShapeDtypeStruct((hp, width), bf)] * 2
    out_shape.append(jax.ShapeDtypeStruct((rows, tot * hp), bf))
    args = [blk, x, inv, w, *pieces, *shared_pieces, *(prev or [token])]
    specs = [SMEM, VMEM, VMEM, VMEM] + [ANY] * (len(args) - 4)
    aliases = {len(args) - 2: 0, len(args) - 1: 1} if prev else {}
    return pl.pallas_call(
        functools.partial(gu_body, n, lo, count, shared, not prev),
        in_specs=specs,
        out_specs=[ANY] * (len(out_shape) - 1) + [VMEM],
        out_shape=out_shape,
        scratch_shapes=[
            pltpu.VMEM((n, 2, tot, hp, df), bf),
            pltpu.VMEM((rows, tot * hp), jnp.float32),
            pltpu.VMEM((rows, tot * hp), jnp.float32),
            pltpu.SemaphoreType.DMA((n, 3)),
            pltpu.SemaphoreType.DMA((n, 2, 2)),
        ],
        input_output_aliases=aliases,
        compiler_params=pltpu.CompilerParams(vmem_limit_bytes=VMEM_LIMIT),
    )(*args)


def down_body(n, parts, lo, count, skip, first, last, *refs):
    refs = list(refs)
    take = lambda k: [refs.pop(0) for _ in range(k)]
    from_ref, blk_ref = take(2)
    gathered = take(parts)
    (acc_in,) = take(1)
    pieces = take(n)
    if not first and not last:
        take(1)
    (down_out,) = [None] if last else take(1)
    results = take(n) if last else take(1)
    buf, a_buf, acc, in_sem, a_sem, out_sem = refs
    share = parts // n
    _, _, hp, dp = buf.shape
    lanes = count * hp
    copies = []
    for s in range(n):
        for j in range(share):
            part = blk_ref[s] * share + j
            rows = pieces[s].at[:, pl.ds(j * hp, hp), :]
            copies.append(pltpu.make_async_copy(rows, buf.at[part], in_sem.at[s, j]))
    for k in range(parts):
        source = gathered[k].at[:, pl.ds(skip * hp, lanes)]
        copies.append(pltpu.make_async_copy(source, a_buf.at[from_ref[k]], a_sem.at[k]))
    copies.append(pltpu.make_async_copy(acc_in, acc, a_sem.at[parts]))
    for copy in copies:
        copy.start()
    for copy in copies:
        copy.wait()
    out = []
    for p in range(0 if last else parts):
        rows = down_out.at[pl.ds(lo, count), pl.ds(p * hp, hp), :]
        out.append(pltpu.make_async_copy(buf.at[p], rows, out_sem.at[p]))
    for copy in out:
        copy.start()
    left = jnp.concatenate([a_buf[p] for p in range(parts)], axis=1)
    right = buf[...].reshape(parts * lanes, dp)
    total = acc[...] + jnp.dot(left, right, preferred_element_type=jnp.float32)
    own = acc.shape[0] // n
    if last:
        for r in range(n):
            results[r][...] = total[r * own : (r + 1) * own].astype(results[r].dtype)
    else:
        results[0][...] = total
    for copy in out:
        copy.wait()


def down_body_narrow(n, parts, lo, count, skip, first, last, *refs):
    refs = list(refs)
    take = lambda k: [refs.pop(0) for _ in range(k)]
    from_ref, blk_ref = take(2)
    gathered = take(parts)
    (acc_in,) = take(1)
    pieces = take(n)
    if not first and not last:
        take(1)
    (down_out,) = [None] if last else take(1)
    results = take(n) if last else take(1)
    buf, in_sem, out_sem = refs
    hf = pieces[0].shape[1]
    copies = []
    for s in range(n):
        rows = pl.ds(pl.multiple_of(blk_ref[s] * hf, hf), hf)
        copies.append(pltpu.make_async_copy(pieces[s], buf.at[:, rows], in_sem.at[s]))
    for copy in copies:
        copy.start()
    for copy in copies:
        copy.wait()
    if not last:
        out = pltpu.make_async_copy(buf, down_out.at[pl.ds(lo, count)], out_sem)
        out.start()
    hp = buf.shape[1] // parts
    dp = buf.shape[2]
    lanes = slice(skip * hp, (skip + count) * hp)
    own = acc_in.shape[0] // n
    for r in range(n):
        at = pl.ds(r * own, own)
        total = acc_in[at, :]
        for k in range(parts):
            hidden = pl.ds(pl.multiple_of(from_ref[k] * hp, hp), hp)
            w = buf[:, hidden, :].reshape(count * hp, dp)
            total += jnp.dot(gathered[k][at, lanes], w, preferred_element_type=jnp.float32)
        if last:
            results[r][...] = total.astype(results[r].dtype)
        else:
            results[0][at, :] = total
    if not last:
        out.wait()


def down_step(source, blk, gathered, acc, pieces, prev, lo, count, skip, n_local, last):
    n, parts = len(pieces), len(gathered)
    _, hf, dp = pieces[0].shape
    rows = acc.shape[0]
    own = rows // n
    hidden = hf * n
    hp = hidden // parts
    share = parts // n
    first = prev is None
    bf = jnp.bfloat16
    if last:
        out_shape = [jax.ShapeDtypeStruct((own, dp), jnp.float32)]
        out_shape += [jax.ShapeDtypeStruct((own, dp), bf)] * (n - 1)
    else:
        out_shape = [jax.ShapeDtypeStruct((n_local, hidden, dp), bf)]
        out_shape.append(jax.ShapeDtypeStruct((rows, dp), jnp.float32))
    args = [source, blk, *gathered, acc, *pieces] + ([] if first or last else [prev])
    specs = [SMEM] * 2 + [ANY] * (len(args) - 2)
    if count * hp % 128 == 0 and skip * hp % 128 == 0 and share * hp == hf:
        kernel = down_body
        scratch = [
            pltpu.VMEM((parts, count, hp, dp), bf),
            pltpu.VMEM((parts, rows, count * hp), bf),
            pltpu.VMEM((rows, dp), jnp.float32),
            pltpu.SemaphoreType.DMA((n, share)),
            pltpu.SemaphoreType.DMA((parts + 1,)),
            pltpu.SemaphoreType.DMA((parts,)),
        ]
    else:
        kernel = down_body_narrow
        specs[2 : parts + 3] = [VMEM] * (parts + 1)
        scratch = [
            pltpu.VMEM((count, hidden, dp), bf),
            pltpu.SemaphoreType.DMA((n,)),
            pltpu.SemaphoreType.DMA,
        ]
    return pl.pallas_call(
        functools.partial(kernel, n, parts, lo, count, skip, first, last),
        in_specs=specs,
        out_specs=[VMEM] * n if last else [ANY, VMEM],
        out_shape=out_shape,
        scratch_shapes=scratch,
        input_output_aliases={} if first or last else {len(args) - 1: 0},
        compiler_params=pltpu.CompilerParams(vmem_limit_bytes=VMEM_LIMIT),
    )(*args)


def layer(
    n,
    tokens,
    expert_ids,
    affinity,
    norm_gain,
    gate_train,
    up_train,
    down_train,
    shared_gate_train,
    shared_up_train,
    shared_down_train,
):
    bf = jnp.bfloat16
    me = lax.axis_index("fs")
    experts, hp, _ = gate_train.shape
    n_local = experts // n
    width = norm_gain.shape[0] * n
    to = [partner(me, s, n)[0] for s in range(n)]
    blk = jnp.stack([partner(me, s, n)[1] for s in range(n)]).astype(jnp.int32)
    base = (jnp.stack(to) * n_local).astype(jnp.int32)
    gain = norm_gain[None, :]

    def swap(pieces):
        return [pieces[0]] + [exchange(pieces[s], "fs", n, s) for s in range(1, n)]

    token_pieces = swap([tokens] * n)

    shared_gu = (jnp.stack([shared_gate_train, shared_up_train]) * gain).astype(bf)
    if n == 4:
        near = [exchange(shared_gu, "fs", n, s) for s in (1, 2)]
        far = [exchange(near[0][0], "fs", n, 2), exchange(near[1][1], "fs", n, 1)]
        shared_gu = [[shared_gu], *([piece] for piece in near), far]
    else:
        shared_gu = [[piece] for piece in swap([shared_gu] * n)]
    table = jnp.concatenate([expert_ids.astype(jnp.float32).T, affinity.T])
    tables = swap([table] * n)
    chunks = cuts(n_local)
    steps = down_cuts(chunks)
    token = tokens
    gu, down = {}, {}
    for c, (lo, count) in enumerate(chunks):
        *pieces, token = prep_gu(gate_train, up_train, gain, base, lo, count, token)
        gu[c] = swap(pieces)
        if c == 1:
            token = packed = pack(token_pieces, token)
            x_same = gather_z(packed)
    for i, (_, lo, count) in enumerate(steps):
        *pieces, token = prep_down(down_train, base, lo, count, token)
        down[i] = swap(pieces)
        if i == len(steps) - 2:
            first_token = token
    own_shared_down = shared_down_train.astype(bf)
    shared_down = swap([own_shared_down] * n)

    x_all = x_same + swap_core(x_same)
    me = me.astype(jnp.int32)[None]
    source = jnp.stack(gathered_from()).astype(jnp.int32)
    x, w, inv = route(me, source, x_all, tables, n_local, hp)
    prev, gathered = [], []
    for c, (lo, count) in enumerate(chunks):
        results = gu_step(
            *(blk, x, inv, w, gu[c], shared_gu if c == 0 else []),
            *(prev, first_token, lo, count, n_local, width),
        )
        if c == 0:
            shared_gate_serve, shared_up_serve = results[2:4]
        prev = results[:2]
        same = gather_z(results[-1])
        gathered.append(same + swap_core(same))
    gate_serve, up_serve = prev

    acc = shared_down_part(n, me, source, gathered[0], own_shared_down)
    down_serve = None
    for i, (c, lo, count) in enumerate(steps):
        last = i == len(steps) - 1
        results = down_step(
            *(source, blk, gathered[c], acc, down[i], down_serve),
            *(lo, count, lo - chunks[c][0], n_local, last),
        )
        if not last:
            down_serve, acc = results
    sums = list(results)
    back = [give_back(sums[s], "fs", n, s) for s in range(1, n)]
    down_serve, shared_down_serve = finish(
        blk, down[len(steps) - 1], shared_down, down_serve, sums[0], steps[-1][1]
    )
    total = sums[0]
    for part in back:
        total = total + part.astype(jnp.float32)
    return (
        total.astype(bf),
        gate_serve,
        up_serve,
        down_serve,
        shared_gate_serve,
        shared_up_serve,
        shared_down_serve,
    )


def body(n, *args):
    return layer(n, *args)


def solution(mesh):
    n = mesh.shape["fs"]
    return jax.shard_map(
        functools.partial(body, n),
        mesh=mesh,
        in_specs=(
            P("fs", "tp"),
            P("fs", None),
            P("fs", None),
            P("fs"),
            P(None, "tp", "fs"),
            P(None, "tp", "fs"),
            P(None, "fs", "tp"),
            P("tp", "fs"),
            P("tp", "fs"),
            P("fs", "tp"),
        ),
        out_specs=(
            P("fs", "tp"),
            P("fs", "tp", None),
            P("fs", "tp", None),
            P("fs", None, "tp"),
            P("tp", None),
            P("tp", None),
            P(None, "tp"),
        ),
        check_vma=False,
    )
```
